128 devices in a mesh: ep: 128 (over z, y, x, core).
Axes of the slice: x: 4, y: 4, z: 4, core: 2. Of those that a mesh axis runs over, the one named last changes fastest.
Arguments:
- tokens: bfloat16 [2560, 2048], P('ep'), may hold values from -6 to 6
- positions: int32 [2560], P('ep'), may hold values from 1024 to 16383
- state: float32 [2560, 8, 64, 128], P('ep'), may hold values from -1.6 to 1.6
- mix_gain: float32 [2048], replicated, may hold values from 0.1 to 1.9
- w_query: bfloat16 [2048, 512], replicated, may hold values from -0.125 to 0.125
- w_key: bfloat16 [2048, 512], replicated, may hold values from -0.125 to 0.125
- w_value: bfloat16 [2048, 1024], replicated, may hold values from -0.125 to 0.125
- ret_gain: float32 [1024], replicated, may hold values from 0.1 to 1.9
- w_out: bfloat16 [1024, 2048], P(None, 'ep'), may hold values from -0.1875 to 0.1875
- ffn_gain: float32 [2048], replicated, may hold values from 0.1 to 1.9
- routes: int32 [2560, 6], P('ep'), may hold values from 0 to 127, all different within a row; in each aligned block of 20 rows (0 to 19, 20 to 39, ...) at most 2 rows name the same one
- route_weights: float32 [2560, 6], P('ep'), may hold values from 0.1 to 1
- expert_gate: bfloat16 [128, 2048, 512], P('ep'), may hold values from -0.125 to 0.125
- expert_up: bfloat16 [128, 2048, 512], P('ep'), may hold values from -0.125 to 0.125
- expert_down: bfloat16 [128, 512, 2048], P('ep'), may hold values from -0.25 to 0.25
Outputs:
- result: bfloat16 [2560, 2048], P('ep')
- new_state: float32 [2560, 8, 64, 128], P('ep')
The draws below stay inside these ranges and needn't reach their ends.
Inputs may be any that keep to these rules, and one draw needn't show every extreme that they name: `routes`: each row names 6 different experts; among the rows of one device no expert is named more than 2 times, a bound that some block reaches there.
All inputs are finite; a program needn't handle non-finite values.
Results may differ from the reference program's by a relative error of at most 0.017.
Values may be sent and summed in bfloat16 or wider, within the bound.
A program may use at most 128 MiB of HBM per device.

```python
import math
import jax
import jax.numpy as jnp
import numpy as np
from jax import lax

D = 2048
HEADS = 8
HEAD_K = 64
HEAD_V = 128
FE = 512
TOPK = 6
SEQ_DEV = 20
QK = 512
VW = 1024
EXPERTS = 128
CAP = 2
TOKENS = 2560
N_EP = 128


def touch_ends(values, own_key, smallest, top_value):
    longest = values.shape.index(max(values.shape))
    spots = []
    for shift in (0, 1):
        where = [jax.random.randint(jax.random.fold_in(own_key, axis), (), 0, length) for axis, length in enumerate(values.shape)]
        where[longest] = (where[longest] + shift) % values.shape[longest]
        spots.append(tuple(where))
    return values.at[spots[0]].set(smallest).at[spots[1]].set(top_value)


def shard_levels(rng, extent, pieces, smallest, high):
    level = 1.0
    for dim, blocks in pieces:
        heights = jax.random.uniform(jax.random.fold_in(jax.random.fold_in(rng, 6), dim), (blocks,), jnp.float32, smallest / len(pieces), high / len(pieces))
        level = level * jnp.repeat(jnp.exp(heights), extent[dim] // blocks).reshape((-1,) + (1,) * (len(extent) - 1 - dim))
    return level


def assign_block(stream_key, own, number, rows, count, top, bound, skew):
    order = jax.random.permutation(stream_key, count)
    crowded, common = portions_of(count, rows * top, bound, skew, True), portions_of(count, rows * top, bound, skew, False)
    places = jnp.arange(count)

    def named(sizes, rotation):
        used = int((sizes > 0).sum())
        fixed = max(1, used // 4)
        passed = fixed + (places - fixed + rotation * (used - fixed)) % max(1, count - fixed)
        return jnp.zeros((count,), jnp.int32).at[order[jnp.where(places < fixed, places, passed)]].set(jnp.asarray(sizes, jnp.int32))

    sizes = jnp.where(number % 4 == 0, named(crowded, number // 4), named(common, number - number // 4 - 1))
    mixed = jax.random.permutation(jax.random.fold_in(own, 3), count)
    donor, receiver = mixed[0:count // 2 * 2:2], mixed[1:count // 2 * 2:2]
    margin = jnp.minimum(sizes[donor] - 1, bound - sizes[receiver]) // 2
    margin = jnp.where((donor == order[0]) | (receiver == order[0]) | (sizes[receiver] == 0), 0, jnp.maximum(margin, 0))
    passed = jax.random.randint(jax.random.fold_in(own, 4), (count // 2,), 0, 1 << 20) % (margin + 1)
    sizes = sizes.at[donor].add(-passed).at[receiver].add(passed)
    items = jnp.searchsorted(jnp.cumsum(sizes), jnp.arange(rows * top), side="right").astype(jnp.int32)
    listing = items.reshape(top, rows).T
    listing = listing[jax.random.permutation(jax.random.fold_in(own, 1), rows)]
    rotation = jax.random.randint(jax.random.fold_in(own, 2), (rows, 1), 0, top)
    return jnp.take_along_axis(listing, (jnp.arange(top)[None, :] + rotation) % top, axis=1)


def portions_of(amount, total, limit, lean, full):
    weights = [(1 << 20) // math.isqrt(standing ** lean) + 1 for standing in range(1, amount + 1)]
    largest = limit if full else min(limit, max(-(-total // amount), total * weights[0] // sum(weights)))
    least = 1 if total - largest >= amount - 1 else 0
    given, spare = [largest] + [least] * (amount - 1), total - largest - least * (amount - 1)
    while spare > 0:
        free = [i for i in range(1, amount) if given[i] < largest] or [i for i in range(1, amount) if given[i] < limit]
        mass, remaining = sum([weights[i] for i in free]), spare
        for i in free:
            extra = min(limit - given[i], max(1, remaining * weights[i] // mass), spare)
            given[i] = given[i] + extra
            spare = spare - extra
    return np.array(given)


def bell_draw(key, shape, spread, reach, cuts=(), held_as=jnp.bfloat16):
    values = jax.random.normal(key, shape, jnp.float32) * spread
    if len(cuts) > 0:
        values = shard_levels(key, shape, cuts, -0.22, 0.18) * values
    return jnp.clip(values, min=-reach, max=reach).astype(held_as)


def setup_inputs(seed: int = 0) -> dict:
    key_list = jax.random.split(jax.random.key(seed), 16)
    tokens = bell_draw(key_list[0], (TOKENS, D), 1.0, 6.0, ((0, 128),))
    positions = touch_ends(jax.random.randint(key_list[1], (TOKENS,), 1024, 16384), jax.random.fold_in(key_list[1], 1), 1024, 16383).astype(jnp.int32)
    state = bell_draw(key_list[2], (TOKENS, HEADS, HEAD_K, HEAD_V), 0.2, 1.6, ((0, 128),), jnp.float32)
    mix_gain = jnp.clip(1.0 + 0.18 * jax.random.normal(key_list[3], (D,), jnp.float32), 0.1, 1.9)
    w_query = bell_draw(key_list[4], (D, QK), D ** -0.5, 0.125)
    w_key = bell_draw(key_list[5], (D, QK), D ** -0.5, 0.125)
    w_value = bell_draw(key_list[6], (D, VW), D ** -0.5, 0.125)
    ret_gain = jnp.clip(1.0 + 0.18 * jax.random.normal(key_list[7], (VW,), jnp.float32), 0.1, 1.9)
    w_out = bell_draw(key_list[8], (VW, D), VW ** -0.5, 0.1875, ((1, 128),))
    ffn_gain = jnp.clip(1.0 + 0.18 * jax.random.normal(key_list[9], (D,), jnp.float32), 0.1, 1.9)
    routes_keys = jax.random.split(jax.random.fold_in(key_list[10], 1), TOKENS // SEQ_DEV)
    routes_turns = jax.random.permutation(jax.random.fold_in(key_list[10], 3), TOKENS // SEQ_DEV)
    routes = jax.vmap(lambda own, number: assign_block(jax.random.fold_in(key_list[10], 2), own, number, SEQ_DEV, EXPERTS, TOPK, CAP, 1))(routes_keys, routes_turns).reshape((TOKENS, TOPK))
    route_weights = jnp.clip(0.1 + 0.9 * jax.random.uniform(key_list[11], (TOKENS, TOPK), jnp.float32) ** shard_levels(key_list[11], (TOKENS, TOPK), ((0, 128),), -0.2, 0.2), 0.1, 1.0)
    expert_gate = bell_draw(key_list[12], (EXPERTS, D, FE), D ** -0.5, 0.125, ((0, 128),))
    expert_up = bell_draw(key_list[13], (EXPERTS, D, FE), D ** -0.5, 0.125, ((0, 128),))
    expert_down = bell_draw(key_list[14], (EXPERTS, FE, D), FE ** -0.5, 0.25, ((0, 128),))
    return {"tokens": tokens, "positions": positions, "state": state, "mix_gain": mix_gain, "w_query": w_query, "w_key": w_key, "w_value": w_value, "ret_gain": ret_gain, "w_out": w_out, "ffn_gain": ffn_gain, "routes": routes, "route_weights": route_weights, "expert_gate": expert_gate, "expert_up": expert_up, "expert_down": expert_down}


EPS = 1e-06

def rms_scale(values, gain):
    wide = values.astype(jnp.float32)
    scaled = wide * lax.rsqrt(lax.optimization_barrier(jnp.mean(wide * wide, axis=-1, keepdims=True)) + EPS)
    return (scaled * gain.astype(jnp.float32)).astype(jnp.bfloat16)

def rotate(field, spots):
    half = field.shape[-1] // 2
    freqs = jnp.exp(-math.log(10000.0) * jnp.arange(half, dtype=jnp.float32) / half)
    angle = spots.astype(jnp.float32)[:, None] * freqs[None, :]
    cosine = jnp.cos(angle)[:, None, :]
    sine = jnp.sin(angle)[:, None, :]
    first = field[..., :half]
    second = field[..., half:]
    return jnp.concatenate([first * cosine - second * sine, second * cosine + first * sine], axis=-1)

def reference(tokens, positions, state, mix_gain, w_query, w_key, w_value, ret_gain, w_out, ffn_gain, routes, route_weights, expert_gate, expert_up, expert_down):
    normed_in = rms_scale(tokens, mix_gain)
    q_proj = jnp.dot(normed_in, w_query, preferred_element_type=jnp.float32).astype(jnp.bfloat16)
    k_proj = jnp.dot(normed_in, w_key, preferred_element_type=jnp.float32).astype(jnp.bfloat16)
    v_proj = jnp.dot(normed_in, w_value, preferred_element_type=jnp.float32).astype(jnp.bfloat16)
    queries = rotate(q_proj.astype(jnp.float32).reshape(TOKENS, HEADS, HEAD_K), positions)
    key_rows = rotate(k_proj.astype(jnp.float32).reshape(TOKENS, HEADS, HEAD_K), positions) * HEAD_K ** (-0.5)
    values = v_proj.astype(jnp.float32).reshape(TOKENS, HEADS, HEAD_V)
    decays = 1.0 - jnp.exp2(-2.0 - jnp.arange(HEADS, dtype=jnp.float32))
    new_state = decays[None, :, None, None] * state + key_rows[:, :, :, None] * values[:, :, None, :]
    readout = jnp.einsum('thd,thdv->thv', queries, new_state, precision=lax.Precision.HIGHEST)
    centre = lax.optimization_barrier(jnp.mean(readout, axis=-1, keepdims=True))
    variance = lax.optimization_barrier(jnp.mean(jnp.square(readout - centre), axis=-1, keepdims=True))
    normed = ((readout - centre) * lax.rsqrt(variance + EPS)).reshape(TOKENS, VW) * ret_gain
    mixed = normed.astype(jnp.bfloat16)
    attended = jnp.dot(mixed, w_out, preferred_element_type=jnp.float32).astype(jnp.bfloat16)
    resid = (tokens.astype(jnp.float32) + attended.astype(jnp.float32)).astype(jnp.bfloat16)
    normed_mid = rms_scale(resid, ffn_gain)
    per_dev = SEQ_DEV * TOPK
    chosen = routes.reshape(N_EP, per_dev).astype(jnp.int32)
    matches = (chosen[:, :, None] == jnp.arange(EXPERTS, dtype=jnp.int32)[None, None, :]).astype(jnp.int32)
    places = lax.optimization_barrier(jnp.sum((jnp.cumsum(matches, axis=1) - matches) * matches, axis=-1))
    dev_ids = jnp.arange(N_EP, dtype=jnp.int32)[:, None]
    targets = (chosen * (N_EP * CAP) + dev_ids * CAP + places).reshape(-1).astype(jnp.int32)
    row_ids = jnp.arange(TOKENS * TOPK, dtype=jnp.int32)
    table = jnp.full((EXPERTS * N_EP * CAP,), -1, jnp.int32).at[targets].set(row_ids)
    table = table.reshape(EXPERTS, N_EP * CAP)

    def serve(items):
        gate_w, up_w, down_w, ids = items
        picked = jnp.where(ids[:, None] >= 0, normed_mid[jnp.maximum(ids, 0) // TOPK], jnp.zeros((), jnp.bfloat16))
        picked = picked.astype(jnp.bfloat16)
        gate_part = jnp.dot(picked, gate_w, preferred_element_type=jnp.float32)
        up_part = jnp.dot(picked, up_w, preferred_element_type=jnp.float32)
        hidden = (jax.nn.silu(gate_part) * up_part).astype(jnp.bfloat16)
        return jnp.dot(hidden, down_w, preferred_element_type=jnp.float32).astype(jnp.bfloat16)
    outputs = lax.map(serve, (expert_gate, expert_up, expert_down, table))
    picked_rows = outputs.reshape(-1, D)[targets].astype(jnp.float32)
    mixture = lax.optimization_barrier(jnp.sum(picked_rows.reshape(TOKENS, TOPK, D) * route_weights[:, :, None], axis=1))
    result = (resid.astype(jnp.float32) + mixture).astype(jnp.bfloat16)
    return (result, new_state)
```

```python
import math

import jax
import jax.numpy as jnp
from jax import lax
from jax.experimental import pallas as pl
from jax.experimental.pallas import tpu as pltpu
from jax.sharding import PartitionSpec as P

MESH = pl.DeviceIdType.MESH
EPS = 1e-06
BF = jnp.bfloat16
F32 = jnp.float32
CUTS = ((0, 384), (384, 768), (768, 1024))
STRIDES = (32, 8, 2)
ORDERS = ((0, 1, 2), (1, 2, 0), (2, 0, 1))


def kernel(
    tokens, pos, mixg, retg, ffng, routes_t, rw_t,
    state, wq, wk, wv, wo, eg, eu, ed,
    result, new_state,
    sbuf, wqv, wkv, wvv, wh, egv, euv, edv,
    xin, tab, kt, qt, vt, rt, mix, mix_in, att, att_in, nm, dmask, chl, rsd, xs, hid,
    send1, recv1, send2, recv2,
    lsem, ssem_in, ssem_out, ag_s, ag_r, ps, pr, a_s, a_r, b_s, b_r,
):
    me = lax.axis_index("ep")
    co = (me // 32, (me // 8) % 4, (me // 2) % 4)
    c = me % 2
    chip = me // 2
    partner = me + 1 - 2 * c
    n_tok = tokens.shape[0]

    cp_wo = pltpu.make_async_copy(wo, wh.at[chip], lsem.at[0])
    cp_wo.start()
    cp_q = pltpu.make_async_copy(wq, wqv, lsem.at[1])
    cp_k = pltpu.make_async_copy(wk, wkv, lsem.at[2])
    cp_v = pltpu.make_async_copy(wv, wvv, lsem.at[3])
    cp_k.start()
    cp_q.start()
    cp_v.start()

    def state_in(h):
        return pltpu.make_async_copy(state.at[:, h], sbuf.at[h], ssem_in.at[h])

    def state_out(h):
        return pltpu.make_async_copy(sbuf.at[h], new_state.at[:, h], ssem_out.at[h])

    for h in range(8):
        state_in(h).start()
    cp_g = pltpu.make_async_copy(eg.at[0], egv, lsem.at[4])
    cp_u = pltpu.make_async_copy(eu.at[0], euv, lsem.at[5])
    cp_d = pltpu.make_async_copy(ed.at[0], edv, lsem.at[6])
    cp_g.start()
    cp_u.start()
    cp_d.start()

    def along(axis, d):
        return me + ((co[axis] + d) % 4 - co[axis]) * STRIDES[axis]

    bar = pltpu.get_barrier_semaphore()
    pl.semaphore_signal(bar, inc=1, device_id=(partner,), device_id_type=MESH)
    for axis in range(3):
        for d in (1, 2, 3):
            pl.semaphore_signal(bar, inc=1, device_id=(along(axis, d),), device_id_type=MESH)

    wide = tokens[...].astype(F32)
    scaled = wide * lax.rsqrt(jnp.mean(wide * wide, axis=-1, keepdims=True) + EPS)
    xin[...] = jnp.zeros(xin.shape, BF)
    xin[0:n_tok, :] = (scaled * mixg[...]).astype(BF)

    tab[...] = jnp.full(tab.shape, -1, jnp.int32)
    tab[0:6, 0:n_tok] = routes_t[...]
    tab[8:9, 0:n_tok] = pos[...]
    wtab = jnp.concatenate([rw_t[...], jnp.zeros((6, 128 - n_tok), F32)], axis=1)
    rows = lax.broadcasted_iota(jnp.int32, (256, 128), 0)
    expert = rows // 2
    slot = (rows % 2).astype(F32)
    member = jnp.zeros((256, 128), F32)
    weight = jnp.zeros((256, 128), F32)
    for k in range(6):
        hit = tab[k : k + 1, :] == expert
        member = member + jnp.where(hit, 1.0, 0.0)
        weight = weight + jnp.where(hit, wtab[k : k + 1, :], 0.0)
    before = jnp.where(
        lax.broadcasted_iota(jnp.int32, (128, 128), 0) < lax.broadcasted_iota(jnp.int32, (128, 128), 1), 1.0, 0.0
    ).astype(BF)
    place = jnp.dot(member.astype(BF), before, preferred_element_type=F32)
    chosen = jnp.where(place == slot, member, 0.0)
    dmask[...] = chosen.astype(BF)
    comb = (chosen * weight).T
    high = comb.astype(BF)
    chl[0:32, :] = high[0:32, :]
    chl[32:64, :] = (comb - high.astype(F32)).astype(BF)[0:32, :]

    spots = tab[8:9, 0:32].astype(F32)
    freqs = jnp.exp(-math.log(10000.0) * lax.broadcasted_iota(jnp.int32, (32, 32), 0).astype(F32) / 32.0)
    angle = spots * freqs
    cosine = jnp.cos(angle)
    sine = jnp.sin(angle)

    def send_block(cc, j, phase):
        axis = ORDERS[j][phase]
        where = (cc[0] * 4 + cc[1]) * 4 + cc[2]
        piece = wh.at[where, :, pl.ds(CUTS[j][0], CUTS[j][1] - CUTS[j][0])]
        for d in (1, 3, 2):
            pltpu.make_async_remote_copy(
                src_ref=piece, dst_ref=piece, send_sem=ag_s, recv_sem=ag_r.at[phase, j],
                device_id=(along(axis, d),), device_id_type=MESH,
            ).start()

    def wait_phase(phase, j):
        n = 3 * 4**phase
        seen = wh.at[pl.ds(0, n), :, pl.ds(CUTS[j][0], CUTS[j][1] - CUTS[j][0])]
        pltpu.make_async_copy(seen, seen, ag_r.at[phase, j]).wait()

    pl.semaphore_wait(bar, 10)
    cp_wo.wait()
    for j in range(3):
        for phase in range(3):
            send_block(co, j, phase)

    def project(wref, n):
        return jnp.dot(xin[...], wref[:, n * 256 : (n + 1) * 256], preferred_element_type=F32).astype(BF).astype(F32)

    def rotated(dst, wref, scale):
        for n in range(2):
            cols = project(wref, n).T
            for s in range(4):
                a = cols[s * 64 : s * 64 + 32, :]
                b = cols[s * 64 + 32 : s * 64 + 64, :]
                dst[n * 4 + s, 0:32, :] = (a * cosine - b * sine) * scale
                dst[n * 4 + s, 32:64, :] = (b * cosine + a * sine) * scale

    cp_k.wait()
    rotated(kt, wkv, 0.125)
    cp_q.wait()
    rotated(qt, wqv, 1.0)

    def forward0():
        for j in range(3):
            wait_phase(0, j)
            a0 = ORDERS[j][0]

            def step(d, _):
                cc = list(co)
                cc[a0] = (co[a0] + d) % 4
                send_block(cc, j, 1)
                send_block(cc, j, 2)
                return 0

            lax.fori_loop(1, 4, step, 0)

    def forward1():
        for j in range(3):
            wait_phase(1, j)
            a0, a1 = ORDERS[j][0], ORDERS[j][1]

            def step(i, _):
                cc = list(co)
                cc[a0] = (co[a0] + i % 4) % 4
                cc[a1] = (co[a1] + 1 + i // 4) % 4
                send_block(cc, j, 2)
                return 0

            lax.fori_loop(0, 12, step, 0)

    forward0()
    cp_v.wait()
    for n in range(4):
        part = project(wvv, n)
        vt[2 * n] = part[:, 0:128]
        vt[2 * n + 1] = part[:, 128:256]

    def head(h, power):
        state_in(h).wait()
        decay = 1.0 - power
        for t in range(n_tok):
            new = decay * sbuf[h, t] + kt[h, :, t : t + 1] * vt[h, t : t + 1, :]
            sbuf[h, t] = new
            rt[h, t : t + 1, :] = jnp.sum(qt[h, :, t : t + 1] * new, axis=0, keepdims=True)
        state_out(h).start()
        return power * 0.5

    power = lax.fori_loop(0, 3, head, jnp.float32(0.25))
    forward1()
    lax.fori_loop(3, 8, head, power)

    for h in range(8):
        read = rt[h, 0:n_tok, :]
        centred = read - jnp.mean(read, axis=-1, keepdims=True)
        normed = centred * lax.rsqrt(jnp.mean(centred * centred, axis=-1, keepdims=True) + EPS)
        mix[0:n_tok, h * 128 : (h + 1) * 128] = (normed * retg[:, h * 128 : (h + 1) * 128]).astype(BF)

    to_partner = pltpu.make_async_remote_copy(
        src_ref=mix, dst_ref=mix_in, send_sem=ps.at[0], recv_sem=pr.at[0], device_id=(partner,), device_id_type=MESH
    )
    to_partner.start()
    nm[...] = jnp.zeros(nm.shape, BF)

    srow = lax.broadcasted_iota(jnp.int32, (256, 256), 0)
    scol = lax.broadcasted_iota(jnp.int32, (256, 256), 1)
    owner = jnp.where(srow < 128, c, 1 - c)
    target = ((srow % 128) // 16) * 32 + owner * 16 + srow % 16
    spread = jnp.where(scol == target, 1.0, 0.0).astype(BF)

    to_partner.wait()
    for j in range(3):
        wait_phase(2, j)
    both = jnp.concatenate([mix[...], mix_in[...]], axis=0)
    for n in range(4):
        block = wh[n * 16 : (n + 1) * 16].reshape(256, 1024)
        att[:, n * 256 : (n + 1) * 256] = lax.dot_general(
            both, block, (((1,), (1,)), ((), ())), preferred_element_type=F32
        ).astype(BF)
    swap = pltpu.make_async_remote_copy(
        src_ref=att.at[pl.ds(32, 32)], dst_ref=att_in, send_sem=ps.at[1], recv_sem=pr.at[1],
        device_id=(partner,), device_id_type=MESH,
    )
    swap.start()
    swap.wait()
    total = jnp.zeros((n_tok, 1), F32)
    for n in range(8):
        halves = jnp.concatenate([att[0:32, n * 128 : (n + 1) * 128], att_in[:, n * 128 : (n + 1) * 128]], axis=1)
        attended = jnp.dot(halves, spread, preferred_element_type=F32)
        cols = slice(n * 256, (n + 1) * 256)
        res = (tokens[:, cols].astype(F32) + attended[0:n_tok, :]).astype(BF).astype(F32)
        rsd[:, cols] = res
        total = total + jnp.sum(res * res, axis=-1, keepdims=True)
    inv = lax.rsqrt(total / 2048.0 + EPS)
    nm[0:n_tok, :] = (rsd[...] * inv * ffng[...]).astype(BF)

    for n in range(8):
        cols = slice(n * 256, (n + 1) * 256)
        out = jnp.dot(dmask[:, 0:32], nm[:, cols], preferred_element_type=F32).astype(BF)
        send1[:, :, cols] = out.reshape(128, 2, 256)

    def exchange(src, dst, ss, rs):
        def body(i, _):
            j = (i * 37) % 128
            t = ((co[0] + j // 32) % 4) * 32 + ((co[1] + (j // 8) % 4) % 4) * 8 + ((co[2] + (j // 2) % 4) % 4) * 2 + (c + j) % 2
            pltpu.make_async_remote_copy(
                src_ref=src.at[t], dst_ref=dst.at[me], send_sem=ss, recv_sem=rs, device_id=(t,), device_id_type=MESH
            ).start()
            return 0

        lax.fori_loop(1, 128, body, 0)
        dst[me] = src[me]

    def finish(src, dst, ss, rs):
        a = dst.at[pl.ds(0, 127)]
        pltpu.make_async_copy(a, a, rs).wait()
        b = src.at[pl.ds(0, 127)]
        pltpu.make_async_copy(b, b, ss).wait()

    exchange(send1, recv1, a_s, a_r)
    cp_g.wait()
    cp_u.wait()
    cp_d.wait()
    finish(send1, recv1, a_s, a_r)

    def unpack(i, _):
        xs[pl.ds(i * 16, 16), :] = recv1[pl.ds(i * 8, 8)].reshape(16, 2048)
        return 0

    lax.fori_loop(0, 16, unpack, 0)
    for n in range(2):
        cols = slice(n * 256, (n + 1) * 256)
        gate = jnp.dot(xs[...], egv[:, cols], preferred_element_type=F32)
        up = jnp.dot(xs[...], euv[:, cols], preferred_element_type=F32)
        hid[:, cols] = (jax.nn.silu(gate) * up).astype(BF)
    for n in range(8):
        cols = slice(n * 256, (n + 1) * 256)
        out = jnp.dot(hid[...], edv[:, cols], preferred_element_type=F32).astype(BF)
        send2[:, :, cols] = out.reshape(128, 2, 256)

    exchange(send2, recv2, b_s, b_r)
    finish(send2, recv2, b_s, b_r)

    def unpack2(i, _):
        xs[pl.ds(i * 16, 16), :] = recv2[pl.ds(i * 8, 8)].reshape(16, 2048)
        return 0

    lax.fori_loop(0, 16, unpack2, 0)
    for n in range(8):
        cols = slice(n * 256, (n + 1) * 256)
        got = jnp.dot(chl[...], xs[:, cols], preferred_element_type=F32)
        result[:, cols] = (rsd[:, cols] + got[0:n_tok, :] + got[32 : 32 + n_tok, :]).astype(BF)

    sent = wh.at[pl.ds(0, 63)]
    pltpu.make_async_copy(sent, sent, ag_s).wait()

    def drain(h, _):
        state_out(h).wait()
        return 0

    lax.fori_loop(0, 8, drain, 0)


def shards(
    tokens, positions, state, mix_gain, w_query, w_key, w_value, ret_gain, w_out, ffn_gain,
    routes, route_weights, expert_gate, expert_up, expert_down,
):
    vmem = pl.BlockSpec(memory_space=pltpu.VMEM)
    hbm = pl.BlockSpec(memory_space=pl.ANY)
    n_tok = tokens.shape[0]
    dma = pltpu.SemaphoreType.DMA
    vm = pltpu.VMEM
    return pl.pallas_call(
        kernel,
        out_shape=(
            jax.ShapeDtypeStruct(tokens.shape, BF),
            jax.ShapeDtypeStruct(state.shape, F32),
        ),
        in_specs=[vmem] * 7 + [hbm] * 8,
        out_specs=(vmem, hbm),
        scratch_shapes=[
            vm((8, n_tok, 64, 128), F32), vm((2048, 512), BF), vm((2048, 512), BF), vm((2048, 1024), BF),
            vm((64, 16, 1024), BF), vm((2048, 512), BF), vm((2048, 512), BF), vm((512, 2048), BF),
            vm((32, 2048), BF), vm((16, 128), jnp.int32), vm((8, 64, 32), F32), vm((8, 64, 32), F32),
            vm((8, 32, 128), F32), vm((8, 32, 128), F32), vm((32, 1024), BF), vm((32, 1024), BF),
            vm((64, 1024), BF), vm((32, 1024), BF), vm((32, 2048), BF), vm((256, 128), BF), vm((64, 256), BF),
            vm((n_tok, 2048), F32), vm((256, 2048), BF), vm((256, 512), BF),
            vm((128, 2, 2048), BF), vm((128, 2, 2048), BF), vm((128, 2, 2048), BF), vm((128, 2, 2048), BF),
            dma((7,)), dma((8,)), dma((8,)), dma, dma((3, 3)), dma((2,)), dma((2,)), dma, dma, dma, dma,
        ],
        compiler_params=pltpu.CompilerParams(collective_id=0, has_side_effects=True, vmem_limit_bytes=56 << 20),
        name="layer",
    )(
        tokens, positions.reshape(1, n_tok), mix_gain.reshape(1, -1), ret_gain.reshape(1, -1), ffn_gain.reshape(1, -1),
        routes.T, route_weights.T, state, w_query, w_key, w_value, w_out.T, expert_gate, expert_up, expert_down,
    )


def solution(mesh):
    placed = (
        P("ep", None), P("ep"), P("ep", None, None, None), P(), P(), P(), P(), P(), P(None, "ep"), P(),
        P("ep", None), P("ep", None), P("ep", None, None), P("ep", None, None), P("ep", None, None),
    )
    return jax.shard_map(
        shards, mesh=mesh, in_specs=placed, out_specs=(P("ep", None), P("ep", None, None, None)), check_vma=False
    )
```

```python
import math

import jax
import jax.numpy as jnp
from jax import lax
from jax.experimental import pallas as pl
from jax.experimental.pallas import tpu as pltpu
from jax.sharding import PartitionSpec as P

MESH = pl.DeviceIdType.MESH
EPS = 1e-06
BF = jnp.bfloat16
F32 = jnp.float32
CUTS = ((0, 384), (384, 768), (768, 1024))
STRIDES = (32, 8, 2)
ORDERS = ((0, 1, 2), (1, 2, 0), (2, 0, 1))


def kernel(
    tokens_h, pos_h, mixg_h, retg_h, ffng_h, routes_h, rw_h,
    state, wq, wk, wv, wo, eg, eu, ed,
    result, new_state,
    tokens, pos, mixg, retg, ffng, routes_t, rw_t, wqv, wkv, wvv, wh, egv, euv, edv,
    xin, tab, kt, qt, vt, rt, mix, mix_in, att, att_in, nm, dmask, chl, rsd, xs, hid,
    send1, recv1, send2, recv2,
    lsem, ssem_in, ag_s, ag_r, ps, pr, a_s, a_r, b_s, b_r,
):
    me = lax.axis_index("ep")
    co = (me // 32, (me // 8) % 4, (me // 2) % 4)
    c = me % 2
    chip = me // 2
    partner = me + 1 - 2 * c
    n_tok = tokens.shape[0]

    def along(axis, d):
        return me + ((co[axis] + d) % 4 - co[axis]) * STRIDES[axis]

    bar = pltpu.get_barrier_semaphore()
    pl.semaphore_signal(bar, inc=1, device_id=(partner,), device_id_type=MESH)
    for axis in range(3):
        for d in (1, 2, 3):
            pl.semaphore_signal(bar, inc=1, device_id=(along(axis, d),), device_id_type=MESH)

    def fetch(n, src, dst):
        cp = pltpu.make_async_copy(src, dst, lsem.at[n])
        cp.start()
        return cp

    cp_tok = fetch(7, tokens_h, tokens)
    cp_mixg = fetch(8, mixg_h, mixg)
    cp_rt = fetch(9, routes_h, routes_t)
    cp_rw = fetch(10, rw_h, rw_t)
    cp_pos = fetch(11, pos_h, pos)
    cp_wo = fetch(0, wo, wh.at[chip])
    cp_k = fetch(1, wk, wkv)
    cp_q = fetch(2, wq, wqv)
    cp_v = fetch(3, wv, wvv)

    def state_in(h):
        return pltpu.make_async_copy(state.at[:, h], new_state.at[:, h], ssem_in.at[h])

    for h in range(8):
        state_in(h).start()
    cp_retg = fetch(12, retg_h, retg)
    cp_ffng = fetch(13, ffng_h, ffng)
    cp_g = fetch(4, eg.at[0], egv)
    cp_u = fetch(5, eu.at[0], euv)
    cp_d = fetch(6, ed.at[0], edv)
    cp_rt.wait()
    cp_rw.wait()
    cp_pos.wait()

    tab[...] = jnp.full(tab.shape, -1, jnp.int32)
    tab[0:6, 0:n_tok] = routes_t[...]
    tab[8:9, 0:n_tok] = pos[...]
    wtab = jnp.concatenate([rw_t[...], jnp.zeros((6, 128 - n_tok), F32)], axis=1)
    rows = lax.broadcasted_iota(jnp.int32, (256, 128), 0)
    expert = rows // 2
    slot = (rows % 2).astype(F32)
    member = jnp.zeros((256, 128), F32)
    weight = jnp.zeros((256, 128), F32)
    for k in range(6):
        hit = tab[k : k + 1, :] == expert
        member = member + jnp.where(hit, 1.0, 0.0)
        weight = weight + jnp.where(hit, wtab[k : k + 1, :], 0.0)
    before = jnp.where(
        lax.broadcasted_iota(jnp.int32, (128, 128), 0) < lax.broadcasted_iota(jnp.int32, (128, 128), 1), 1.0, 0.0
    ).astype(BF)
    place = jnp.dot(member.astype(BF), before, preferred_element_type=F32)
    chosen = jnp.where(place == slot, member, 0.0)
    dmask[...] = chosen.astype(BF)
    comb = (chosen * weight).T
    high = comb.astype(BF)
    chl[0:32, :] = high[0:32, :]
    chl[32:64, :] = (comb - high.astype(F32)).astype(BF)[0:32, :]

    spots = tab[8:9, 0:32].astype(F32)
    freqs = jnp.exp(-math.log(10000.0) * lax.broadcasted_iota(jnp.int32, (32, 32), 0).astype(F32) / 32.0)
    angle = spots * freqs
    cosine = jnp.cos(angle)
    sine = jnp.sin(angle)

    cp_tok.wait()
    cp_mixg.wait()
    wide = tokens[...].astype(F32)
    scaled = wide * lax.rsqrt(jnp.mean(wide * wide, axis=-1, keepdims=True) + EPS)
    xin[...] = jnp.zeros(xin.shape, BF)
    xin[0:n_tok, :] = (scaled * mixg[...]).astype(BF)

    def send_block(cc, j, phase):
        axis = ORDERS[j][phase]
        where = (cc[0] * 4 + cc[1]) * 4 + cc[2]
        piece = wh.at[where, :, pl.ds(CUTS[j][0], CUTS[j][1] - CUTS[j][0])]
        for d in (1, 3, 2):
            pltpu.make_async_remote_copy(
                src_ref=piece, dst_ref=piece, send_sem=ag_s, recv_sem=ag_r.at[phase, j],
                device_id=(along(axis, d),), device_id_type=MESH,
            ).start()

    def wait_phase(phase, j):
        n = 3 * 4**phase
        seen = wh.at[pl.ds(0, n), :, pl.ds(CUTS[j][0], CUTS[j][1] - CUTS[j][0])]
        pltpu.make_async_copy(seen, seen, ag_r.at[phase, j]).wait()

    pl.semaphore_wait(bar, 10)
    cp_wo.wait()
    for j in range(3):
        for phase in range(3):
            send_block(co, j, phase)

    def project(wref, n):
        return jnp.dot(xin[...], wref[:, n * 256 : (n + 1) * 256], preferred_element_type=F32).astype(BF).astype(F32)

    def rotated(dst, wref, scale):
        for n in range(2):
            cols = project(wref, n).T
            for s in range(4):
                a = cols[s * 64 : s * 64 + 32, :]
                b = cols[s * 64 + 32 : s * 64 + 64, :]
                dst[n * 4 + s, 0:32, :] = (a * cosine - b * sine) * scale
                dst[n * 4 + s, 32:64, :] = (b * cosine + a * sine) * scale

    cp_k.wait()
    rotated(kt, wkv, 0.125)
    cp_q.wait()
    rotated(qt, wqv, 1.0)

    def forward0():
        for j in range(3):
            wait_phase(0, j)
            a0 = ORDERS[j][0]

            def step(d, _):
                cc = list(co)
                cc[a0] = (co[a0] + d) % 4
                send_block(cc, j, 1)
                send_block(cc, j, 2)
                return 0

            lax.fori_loop(1, 4, step, 0)

    def forward1():
        for j in range(3):
            wait_phase(1, j)
            a0, a1 = ORDERS[j][0], ORDERS[j][1]

            def step(i, _):
                cc = list(co)
                cc[a0] = (co[a0] + i % 4) % 4
                cc[a1] = (co[a1] + 1 + i // 4) % 4
                send_block(cc, j, 2)
                return 0

            lax.fori_loop(0, 12, step, 0)

    forward0()
    cp_v.wait()
    for n in range(4):
        part = project(wvv, n)
        vt[2 * n] = part[:, 0:128]
        vt[2 * n + 1] = part[:, 128:256]

    def head(h, power):
        state_in(h).wait()
        decay = 1.0 - power
        for t in range(n_tok):
            new = decay * new_state[t, h] + kt[h, :, t : t + 1] * vt[h, t : t + 1, :]
            new_state[t, h] = new
            rt[h, t : t + 1, :] = jnp.sum(qt[h, :, t : t + 1] * new, axis=0, keepdims=True)
        return power * 0.5

    power = lax.fori_loop(0, 3, head, jnp.float32(0.25))
    forward1()
    lax.fori_loop(3, 8, head, power)

    cp_retg.wait()
    for h in range(8):
        read = rt[h, 0:n_tok, :]
        centred = read - jnp.mean(read, axis=-1, keepdims=True)
        normed = centred * lax.rsqrt(jnp.mean(centred * centred, axis=-1, keepdims=True) + EPS)
        mix[0:n_tok, h * 128 : (h + 1) * 128] = (normed * retg[:, h * 128 : (h + 1) * 128]).astype(BF)

    to_partner = pltpu.make_async_remote_copy(
        src_ref=mix, dst_ref=mix_in, send_sem=ps.at[0], recv_sem=pr.at[0], device_id=(partner,), device_id_type=MESH
    )
    to_partner.start()
    nm[...] = jnp.zeros(nm.shape, BF)

    srow = lax.broadcasted_iota(jnp.int32, (256, 256), 0)
    scol = lax.broadcasted_iota(jnp.int32, (256, 256), 1)
    owner = jnp.where(srow < 128, c, 1 - c)
    target = ((srow % 128) // 16) * 32 + owner * 16 + srow % 16
    spread = jnp.where(scol == target, 1.0, 0.0).astype(BF)

    to_partner.wait()
    for j in range(3):
        wait_phase(2, j)
    both = jnp.concatenate([mix[...], mix_in[...]], axis=0)
    for n in range(4):
        block = wh[n * 16 : (n + 1) * 16].reshape(256, 1024)
        att[:, n * 256 : (n + 1) * 256] = lax.dot_general(
            both, block, (((1,), (1,)), ((), ())), preferred_element_type=F32
        ).astype(BF)
    swap = pltpu.make_async_remote_copy(
        src_ref=att.at[pl.ds(32, 32)], dst_ref=att_in, send_sem=ps.at[1], recv_sem=pr.at[1],
        device_id=(partner,), device_id_type=MESH,
    )
    swap.start()
    swap.wait()
    cp_ffng.wait()
    total = jnp.zeros((n_tok, 1), F32)
    for n in range(8):
        halves = jnp.concatenate([att[0:32, n * 128 : (n + 1) * 128], att_in[:, n * 128 : (n + 1) * 128]], axis=1)
        attended = jnp.dot(halves, spread, preferred_element_type=F32)
        cols = slice(n * 256, (n + 1) * 256)
        res = (tokens[:, cols].astype(F32) + attended[0:n_tok, :]).astype(BF).astype(F32)
        rsd[:, cols] = res
        total = total + jnp.sum(res * res, axis=-1, keepdims=True)
    inv = lax.rsqrt(total / 2048.0 + EPS)
    nm[0:n_tok, :] = (rsd[...] * inv * ffng[...]).astype(BF)

    for n in range(8):
        cols = slice(n * 256, (n + 1) * 256)
        out = jnp.dot(dmask[:, 0:32], nm[:, cols], preferred_element_type=F32).astype(BF)
        send1[:, :, cols] = out.reshape(128, 2, 256)

    def peers(half, sign, put):
        zs = [((co[0] + sign * (half + 2 * i)) % 4) * 32 for i in range(2)]
        xs8 = [((co[2] + sign * dx) % 4) * 2 + (c + dc) % 2 for dx in range(4) for dc in range(2)]

        def row(i, skip):
            zz = jnp.where(i // 4 == 0, zs[0], zs[1])
            base = zz + ((co[1] + sign * (i % 4) + 4) % 4) * 8
            for n in range(8):
                if n >= skip:
                    put(half * 64 + i * 8 + n, base + xs8[n])

        if half == 0:
            row(jnp.int32(0), 1)
        lax.fori_loop(1 - half, 8, lambda i, _: (row(i, 0), 0)[1], 0)

    def dispatch(half):
        def put(j, t):
            pltpu.make_async_remote_copy(
                src_ref=send1.at[t], dst_ref=recv1.at[j], send_sem=a_s, recv_sem=a_r.at[half],
                device_id=(t,), device_id_type=MESH,
            ).start()

        peers(half, 1, put)

    def give_back(half):
        def put(j, t):
            pltpu.make_async_remote_copy(
                src_ref=send2.at[j], dst_ref=recv2.at[me], send_sem=b_s, recv_sem=b_r,
                device_id=(t,), device_id_type=MESH,
            ).start()

        peers(half, -1, put)

    def arrived(buf, first, count, sem):
        seen = buf.at[pl.ds(first, count)]
        pltpu.make_async_copy(seen, seen, sem).wait()

    def experts(half):
        base = half * 128
        for i in range(8):
            xs[base + i * 16 : base + (i + 1) * 16, :] = recv1[half * 64 + i * 8 : half * 64 + (i + 1) * 8].reshape(16, 2048)
        mine = slice(base, base + 128)
        for n in range(2):
            cols = slice(n * 256, (n + 1) * 256)
            gate = jnp.dot(xs[mine, :], egv[:, cols], preferred_element_type=F32)
            up = jnp.dot(xs[mine, :], euv[:, cols], preferred_element_type=F32)
            hid[mine, cols] = (jax.nn.silu(gate) * up).astype(BF)
        for n in range(8):
            cols = slice(n * 256, (n + 1) * 256)
            out = jnp.dot(hid[mine, :], edv[:, cols], preferred_element_type=F32).astype(BF)
            send2[half * 64 : half * 64 + 64, :, cols] = out.reshape(64, 2, 256)

    dispatch(0)
    dispatch(1)
    recv1[0] = send1[me]
    cp_g.wait()
    cp_u.wait()
    cp_d.wait()
    arrived(recv1, 1, 63, a_r.at[0])
    experts(0)
    give_back(0)
    recv2[me] = send2[0]
    arrived(recv1, 64, 64, a_r.at[1])
    experts(1)
    give_back(1)
    arrived(recv2, 0, 127, b_r)

    def unpack2(i, _):
        xs[pl.ds(i * 16, 16), :] = recv2[pl.ds(i * 8, 8)].reshape(16, 2048)
        return 0

    lax.fori_loop(0, 16, unpack2, 0)
    for n in range(8):
        cols = slice(n * 256, (n + 1) * 256)
        got = jnp.dot(chl[...], xs[:, cols], preferred_element_type=F32)
        result[:, cols] = (rsd[:, cols] + got[0:n_tok, :] + got[32 : 32 + n_tok, :]).astype(BF)

    arrived(send1, 0, 127, a_s)
    arrived(send2, 0, 127, b_s)
    sent = wh.at[pl.ds(0, 63)]
    pltpu.make_async_copy(sent, sent, ag_s).wait()


def shards(
    tokens, positions, state, mix_gain, w_query, w_key, w_value, ret_gain, w_out, ffn_gain,
    routes, route_weights, expert_gate, expert_up, expert_down,
):
    vmem = pl.BlockSpec(memory_space=pltpu.VMEM)
    hbm = pl.BlockSpec(memory_space=pl.ANY)
    n_tok = tokens.shape[0]
    dma = pltpu.SemaphoreType.DMA
    vm = pltpu.VMEM
    return pl.pallas_call(
        kernel,
        out_shape=(
            jax.ShapeDtypeStruct(tokens.shape, BF),
            pltpu.VMEM(state.shape, F32),
        ),
        in_specs=[hbm] * 15,
        out_specs=(vmem, vmem),
        scratch_shapes=[
            vm((n_tok, 2048), BF), vm((1, n_tok), jnp.int32), vm((1, 2048), F32), vm((1, 1024), F32), vm((1, 2048), F32),
            vm((6, n_tok), jnp.int32), vm((6, n_tok), F32),
            vm((2048, 512), BF), vm((2048, 512), BF), vm((2048, 1024), BF),
            vm((64, 16, 1024), BF), vm((2048, 512), BF), vm((2048, 512), BF), vm((512, 2048), BF),
            vm((32, 2048), BF), vm((16, 128), jnp.int32), vm((8, 64, 32), F32), vm((8, 64, 32), F32),
            vm((8, 32, 128), F32), vm((8, 32, 128), F32), vm((32, 1024), BF), vm((32, 1024), BF),
            vm((64, 1024), BF), vm((32, 1024), BF), vm((32, 2048), BF), vm((256, 128), BF), vm((64, 256), BF),
            vm((n_tok, 2048), F32), vm((256, 2048), BF), vm((256, 512), BF),
            vm((128, 2, 2048), BF), vm((128, 2, 2048), BF), vm((128, 2, 2048), BF), vm((128, 2, 2048), BF),
            dma((14,)), dma((8,)), dma, dma((3, 3)), dma((2,)), dma((2,)), dma, dma((2,)), dma, dma,
        ],
        compiler_params=pltpu.CompilerParams(collective_id=0, has_side_effects=True, vmem_limit_bytes=61718528),
        name="layer",
    )(
        tokens, positions.reshape(1, n_tok), mix_gain.reshape(1, -1), ret_gain.reshape(1, -1), ffn_gain.reshape(1, -1),
        routes.T, route_weights.T, state, w_query, w_key, w_value, w_out.T, expert_gate, expert_up, expert_down,
    )


def solution(mesh):
    placed = (
        P("ep", None), P("ep"), P("ep", None, None, None), P(), P(), P(), P(), P(), P(None, "ep"), P(),
        P("ep", None), P("ep", None), P("ep", None, None), P("ep", None, None), P("ep", None, None),
    )
    return jax.shard_map(
        shards, mesh=mesh, in_specs=placed, out_specs=(P("ep", None), P("ep", None, None, None)), check_vma=False
    )
```

```python
import math

import jax
import jax.numpy as jnp
from jax import lax
from jax.experimental import pallas as pl
from jax.experimental.pallas import tpu as pltpu
from jax.sharding import PartitionSpec as P

MESH = pl.DeviceIdType.MESH
EPS = 1e-06
BF = jnp.bfloat16
F32 = jnp.float32
STRIDES = (32, 8, 2)


def hops(d):
    return sum((0, 1, 2, 1)[k] for k in d[:3])


MOVES = [(z, y, x, c) for z in range(4) for y in range(4) for x in range(4) for c in range(2)]
MOVES = (lambda r: [(0, 0, 0, 0)] + r[0::2][:63] + r[1::2] + r[0::2][63:])(sorted([d for d in MOVES if d != (0, 0, 0, 0)], key=lambda d: (-hops(d), d)))


def kernel(
    tokens_h, pos_h, mixg_h, retg_h, ffng_h, routes_h, rw_h,
    state, wq, wk, wv, wo, eg, eu, ed,
    result, new_state,
    tokens, pos, mixg, retg, ffng, routes_t, rw_t, wqv, wkv, wvv, wh, egv, euv, edv,
    xin, tab, kq, ee, vt, rt, mix, att, att_in, lined, spread, nm, dmask, chl, rsd, xs, hid,
    send1, recv1, send2, recv2,
    lsem, ssem_in, ag_s, ag_r, ps, pr, a_s, a_r, b_s, b_r,
):
    me = lax.axis_index("ep")
    co = (me // 32, (me // 8) % 4, (me // 2) % 4)
    c = me % 2
    half = (co[0], co[1] // 2, co[2] // 2)
    own = (half[0] * 2 + half[1]) * 2 + half[2]
    n_tok = tokens.shape[0]

    def along(axis, d):
        return ((co[axis] + d) % 4 - co[axis]) * STRIDES[axis]

    line = [(me + along(0, d), ((half[0] + d) % 4, half[1], half[2])) for d in (2, 1, 3)]
    cross = [
        (me + along(1, 2 * fy) + along(2, 2 * fx), (half[0], (half[1] + fy) % 2, (half[2] + fx) % 2))
        for fy, fx in ((1, 1), (1, 0), (0, 1))
    ]

    low = (co[1] % 2, co[2] % 2, c)
    seat = low[0] * 4 + low[1] * 2 + c
    mates = []
    for flip in range(1, 8):
        f = (flip // 4, (flip // 2) % 2, flip % 2)
        there = me + sum(f[a] * (1 - 2 * low[a]) * (8, 2, 1)[a] for a in range(3))
        its_seat = seat + sum(f[a] * (1 - 2 * low[a]) * (4, 2, 1)[a] for a in range(3))
        mates.append((there, its_seat))

    bar = pltpu.get_barrier_semaphore()
    for there, _ in mates:
        pl.semaphore_signal(bar, inc=1, device_id=(there,), device_id_type=MESH)
    for there, _ in line + cross:
        pl.semaphore_signal(bar, inc=1, device_id=(there,), device_id_type=MESH)

    def fetch(n, src, dst):
        cp = pltpu.make_async_copy(src, dst, lsem.at[n])
        cp.start()
        return cp

    cp_tok = fetch(7, tokens_h, tokens)
    cp_mixg = fetch(8, mixg_h, mixg)
    cp_rt = fetch(9, routes_h, routes_t)
    cp_rw = fetch(10, rw_h, rw_t)
    cp_pos = fetch(11, pos_h, pos)
    cp_wo = fetch(0, wo, wh.at[own])
    cp_k = fetch(1, wk, wkv)
    cp_q = fetch(2, wq, wqv)
    cp_v = fetch(3, wv, wvv)

    def state_in(h):
        return pltpu.make_async_copy(state.at[:, h], new_state.at[:, h], ssem_in.at[h])

    for h in range(8):
        state_in(h).start()
    cp_retg = fetch(12, retg_h, retg)
    cp_ffng = fetch(13, ffng_h, ffng)
    cp_g = fetch(4, eg.at[0], egv)
    cp_u = fetch(5, eu.at[0], euv)
    cp_d = fetch(6, ed.at[0], edv)
    cp_rt.wait()
    cp_rw.wait()
    cp_pos.wait()

    tab[...] = jnp.full(tab.shape, -1, jnp.int32)
    tab[0:6, 0:n_tok] = routes_t[...]
    tab[8:9, 0:n_tok] = pos[...]
    wtab = jnp.concatenate([rw_t[...], jnp.zeros((6, 128 - n_tok), F32)], axis=1)
    rows = lax.broadcasted_iota(jnp.int32, (256, 128), 0)
    expert = rows // 2
    slot = (rows % 2).astype(F32)
    member = jnp.zeros((256, 128), F32)
    weight = jnp.zeros((256, 128), F32)
    for k in range(6):
        hit = tab[k : k + 1, :] == expert
        member = member + jnp.where(hit, 1.0, 0.0)
        weight = weight + jnp.where(hit, wtab[k : k + 1, :], 0.0)
    before = jnp.where(
        lax.broadcasted_iota(jnp.int32, (128, 128), 0) < lax.broadcasted_iota(jnp.int32, (128, 128), 1), 1.0, 0.0
    ).astype(BF)
    place = jnp.dot(member.astype(BF), before, preferred_element_type=F32)
    chosen = jnp.where(place == slot, member, 0.0)
    dmask[...] = chosen.astype(BF)
    comb = (chosen * weight).T
    high = comb.astype(BF)
    chl[0:32, :] = high[0:32, :]
    chl[32:64, :] = (comb - high.astype(F32)).astype(BF)[0:32, :]

    erow = lax.broadcasted_iota(jnp.int32, (128, 128), 0)
    etok = jnp.where(erow < 64, erow % 32, -1)
    for t in range(n_tok):
        ee[:, t * 128 : (t + 1) * 128] = jnp.where(etok == t, 1.0, 0.0).astype(BF)

    spots = tab[8:9, 0:32].astype(F32)
    freqs = jnp.exp(-math.log(10000.0) * lax.broadcasted_iota(jnp.int32, (32, 32), 0).astype(F32) / 32.0)
    angle = spots * freqs
    cosine = jnp.cos(angle)
    sine = jnp.sin(angle)

    cp_tok.wait()
    cp_mixg.wait()
    wide = tokens[...].astype(F32)
    scaled = wide * lax.rsqrt(jnp.mean(wide * wide, axis=-1, keepdims=True) + EPS)
    xin[...] = jnp.zeros(xin.shape, BF)
    xin[0:n_tok, :] = (scaled * mixg[...]).astype(BF)

    def send_block(cc, part, peers, sem):
        piece = wh.at[(cc[0] * 2 + cc[1]) * 2 + cc[2], :, pl.ds(part * 512, 512)]
        for there, _ in peers:
            pltpu.make_async_remote_copy(
                src_ref=piece, dst_ref=piece, send_sem=ag_s, recv_sem=ag_r.at[sem],
                device_id=(there,), device_id_type=MESH,
            ).start()

    def gathered(n, sem):
        seen = wh.at[pl.ds(0, n), :, pl.ds(0, 512)]
        pltpu.make_async_copy(seen, seen, ag_r.at[sem]).wait()

    def gather_start():
        send_block(half, 0, line, 0)
        send_block(half, 1, cross, 1)
        send_block(half, 0, cross, 2)
        send_block(half, 1, line, 3)

    def gather_forward():
        gathered(3, 0)
        for _, cc in line:
            send_block(cc, 0, cross, 2)
        gathered(3, 1)
        for _, cc in cross:
            send_block(cc, 1, line, 3)

    def project(wref, n):
        return jnp.dot(xin[...], wref[:, n * 256 : (n + 1) * 256], preferred_element_type=F32).astype(BF).astype(F32)

    def rotated(offset, wref, scale):
        for n in range(2):
            cols = project(wref, n).T
            for s in range(4):
                a = cols[s * 64 : s * 64 + 32, :]
                b = cols[s * 64 + 32 : s * 64 + 64, :]
                for first, value in ((0, a * cosine - b * sine), (32, b * cosine + a * sine)):
                    value = value * scale
                    high = value.astype(BF)
                    low_part = (value - high.astype(F32)).astype(BF)
                    kq[n * 4 + s, offset + first : offset + first + 32, :] = jnp.concatenate(
                        [high, low_part, jnp.zeros((32, 64), BF)], axis=1
                    )

    cp_k.wait()
    rotated(0, wkv, 0.125)
    pl.semaphore_wait(bar, 13)
    cp_wo.wait()
    gather_start()
    cp_q.wait()
    rotated(64, wqv, 1.0)
    cp_v.wait()
    for n in range(4):
        part = project(wvv, n)
        vt[2 * n] = part[:, 0:128]
        vt[2 * n + 1] = part[:, 128:256]

    def seven(buf, sem):
        seen = buf.at[pl.ds(0, 7), pl.ds(0, 24)]
        pltpu.make_async_copy(seen, seen, sem).wait()

    def two_heads(p):
        for h in (2 * p, 2 * p + 1):
            state_in(h).wait()
        lhs = kq[2 * p : 2 * p + 2].reshape(256, 128)
        for g in range(n_tok // 4):
            wide_kq = jnp.dot(lhs, ee[:, g * 512 : (g + 1) * 512], preferred_element_type=F32)
            for n, h in enumerate((2 * p, 2 * p + 1)):
                decay = 1.0 - 2.0 ** (-2 - h)
                for i in range(4):
                    t = g * 4 + i
                    key = wide_kq[n * 128 : n * 128 + 64, i * 128 : (i + 1) * 128]
                    query = wide_kq[n * 128 + 64 : n * 128 + 128, i * 128 : (i + 1) * 128]
                    new = decay * new_state[t, h] + key * vt[h, t : t + 1, :]
                    new_state[t, h] = new
                    rt[h, t : t + 1, :] = jnp.sum(query * new, axis=0, keepdims=True)
        for h in (2 * p, 2 * p + 1):
            read = rt[h, 0:n_tok, :]
            centred = read - jnp.mean(read, axis=-1, keepdims=True)
            normed = centred * lax.rsqrt(jnp.mean(centred * centred, axis=-1, keepdims=True) + EPS)
            mix[seat, 0:n_tok, h * 128 : (h + 1) * 128] = (normed * retg[:, h * 128 : (h + 1) * 128]).astype(BF)
        piece = mix.at[seat, pl.ds(0, 24), pl.ds(p * 256, 256)]
        for n, (there, _) in enumerate([mates[5], mates[3], mates[1], mates[0]]):
            pltpu.make_async_remote_copy(
                src_ref=piece, dst_ref=piece, send_sem=ps.at[0], recv_sem=pr.at[2 + n],
                device_id=(there,), device_id_type=MESH,
            ).start()

    cp_retg.wait()
    two_heads(0)
    two_heads(1)
    two_heads(2)
    gather_forward()
    two_heads(3)
    nm[...] = jnp.zeros(nm.shape, BF)

    srow = lax.broadcasted_iota(jnp.int32, (512, 128), 0)
    lane = lax.broadcasted_iota(jnp.int32, (512, 128), 1)
    target = (srow % 128) // 64 * 256 + (srow % 64) // 32 * 128 + (srow % 32) // 16 * 64 + srow // 128 * 16 + srow % 16
    for n in range(4):
        spread[:, n * 128 : (n + 1) * 128] = jnp.where(lane + n * 128 == target, 1.0, 0.0).astype(BF)

    for n, (_, its_seat) in ((1, mates[3]), (2, mates[1]), (0, mates[5])):
        block = mix.at[0, pl.ds(0, 24)]
        pltpu.make_async_copy(block, block, pr.at[2 + n]).wait()
        block = mix.at[its_seat, pl.ds(0, 24)]
        pltpu.make_async_remote_copy(
            src_ref=block, dst_ref=block, send_sem=ps.at[0], recv_sem=pr.at[0],
            device_id=(mates[0][0],), device_id_type=MESH,
        ).start()
    gathered(12, 2)
    gathered(12, 3)
    block = mix.at[0, pl.ds(0, 24)]
    pltpu.make_async_copy(block, block, pr.at[5]).wait()
    pltpu.make_async_copy(mix.at[pl.ds(0, 3), pl.ds(0, 24)], mix.at[pl.ds(0, 3), pl.ds(0, 24)], pr.at[0]).wait()
    att[...] = lax.dot_general(
        mix[...].reshape(256, 1024), wh[...].reshape(256, 1024), (((1,), (1,)), ((), ())), preferred_element_type=F32
    ).astype(BF).reshape(8, 32, 256)
    for there, its_seat in mates:
        pltpu.make_async_remote_copy(
            src_ref=att.at[its_seat, pl.ds(0, 24)], dst_ref=att_in.at[seat, pl.ds(0, 24)],
            send_sem=ps.at[1], recv_sem=pr.at[1], device_id=(there,), device_id_type=MESH,
        ).start()
    att_in[seat] = att[seat]
    seven(att_in, pr.at[1])
    for py in range(2):
        for zp in range(2):
            for s in range(4):
                lined[(py * 2 + zp) * 32 : (py * 2 + zp + 1) * 32, s * 128 : (s + 1) * 128] = att_in[
                    py * 4 + s, :, zp * 128 : (zp + 1) * 128
                ]
    attended = jnp.dot(lined[...], spread[...], preferred_element_type=F32)
    cp_ffng.wait()
    total = jnp.zeros((n_tok, 1), F32)
    for n in range(16):
        z, y = n // 4, n % 4
        first = (y % 2 * 2 + z // 2) * 32
        at = (z % 2 * 2 + y // 2) * 128
        cols = slice(n * 128, (n + 1) * 128)
        res = (tokens[:, cols].astype(F32) + attended[first : first + n_tok, at : at + 128]).astype(BF).astype(F32)
        rsd[:, cols] = res
        total = total + jnp.sum(res * res, axis=-1, keepdims=True)
    inv = lax.rsqrt(total / 2048.0 + EPS)
    nm[0:n_tok, :] = (rsd[...] * inv * ffng[...]).astype(BF)

    for n in range(8):
        cols = slice(n * 256, (n + 1) * 256)
        out = jnp.dot(dmask[:, 0:32], nm[:, cols], preferred_element_type=F32).astype(BF)
        send1[:, :, cols] = out.reshape(128, 2, 256)

    def peers(half, sign, put):
        zs = [(co[0] + sign * d) % 4 * 32 for d in range(4)]
        ys = [(co[1] + sign * d) % 4 * 8 for d in range(4)]
        xs4 = [(co[2] + sign * d) % 4 * 2 for d in range(4)]
        cs = [c, 1 - c]
        for j in range(max(1, half * 64), half * 64 + 64):
            d = MOVES[j]
            put(j, zs[d[0]] + ys[d[1]] + xs4[d[2]] + cs[d[3]])

    def dispatch(half):
        def put(j, t):
            pltpu.make_async_remote_copy(
                src_ref=send1.at[t], dst_ref=recv1.at[j], send_sem=a_s, recv_sem=a_r.at[half],
                device_id=(t,), device_id_type=MESH,
            ).start()

        peers(half, 1, put)

    def give_back(half):
        def put(j, t):
            pltpu.make_async_remote_copy(
                src_ref=send2.at[j], dst_ref=recv2.at[me], send_sem=b_s, recv_sem=b_r,
                device_id=(t,), device_id_type=MESH,
            ).start()

        peers(half, -1, put)

    def arrived(buf, first, count, sem):
        seen = buf.at[pl.ds(first, count)]
        pltpu.make_async_copy(seen, seen, sem).wait()

    def experts(half):
        base = half * 128
        for i in range(8):
            xs[base + i * 16 : base + (i + 1) * 16, :] = recv1[half * 64 + i * 8 : half * 64 + (i + 1) * 8].reshape(16, 2048)
        mine = slice(base, base + 128)
        for n in range(2):
            cols = slice(n * 256, (n + 1) * 256)
            gate = jnp.dot(xs[mine, :], egv[:, cols], preferred_element_type=F32)
            up = jnp.dot(xs[mine, :], euv[:, cols], preferred_element_type=F32)
            hid[mine, cols] = (jax.nn.silu(gate) * up).astype(BF)
        for n in range(8):
            cols = slice(n * 256, (n + 1) * 256)
            out = jnp.dot(hid[mine, :], edv[:, cols], preferred_element_type=F32).astype(BF)
            send2[half * 64 : half * 64 + 64, :, cols] = out.reshape(64, 2, 256)

    dispatch(0)
    dispatch(1)
    recv1[0] = send1[me]
    cp_g.wait()
    cp_u.wait()
    cp_d.wait()
    arrived(recv1, 1, 63, a_r.at[0])
    experts(0)
    give_back(0)
    recv2[me] = send2[0]
    arrived(recv1, 64, 64, a_r.at[1])
    experts(1)
    give_back(1)
    arrived(recv2, 0, 127, b_r)

    def unpack2(i, _):
        xs[pl.ds(i * 16, 16), :] = recv2[pl.ds(i * 8, 8)].reshape(16, 2048)
        return 0

    lax.fori_loop(0, 16, unpack2, 0)
    for n in range(8):
        cols = slice(n * 256, (n + 1) * 256)
        got = jnp.dot(chl[...], xs[:, cols], preferred_element_type=F32)
        result[:, cols] = (rsd[:, cols] + got[0:n_tok, :] + got[32 : 32 + n_tok, :]).astype(BF)

    arrived(send1, 0, 127, a_s)
    arrived(send2, 0, 127, b_s)
    sent = wh.at[pl.ds(0, 15)]
    pltpu.make_async_copy(sent, sent, ag_s).wait()
    seven(mix, ps.at[0])
    seven(att, ps.at[1])


def shards(
    tokens, positions, state, mix_gain, w_query, w_key, w_value, ret_gain, w_out, ffn_gain,
    routes, route_weights, expert_gate, expert_up, expert_down,
):
    vmem = pl.BlockSpec(memory_space=pltpu.VMEM)
    hbm = pl.BlockSpec(memory_space=pl.ANY)
    n_tok = tokens.shape[0]
    dma = pltpu.SemaphoreType.DMA
    vm = pltpu.VMEM
    return pl.pallas_call(
        kernel,
        out_shape=(
            jax.ShapeDtypeStruct(tokens.shape, BF),
            pltpu.VMEM(state.shape, F32),
        ),
        in_specs=[hbm] * 15,
        out_specs=(vmem, vmem),
        scratch_shapes=[
            vm((n_tok, 2048), BF), vm((1, n_tok), jnp.int32), vm((1, 2048), F32), vm((1, 1024), F32), vm((1, 2048), F32),
            vm((6, n_tok), jnp.int32), vm((6, n_tok), F32),
            vm((2048, 512), BF), vm((2048, 512), BF), vm((2048, 1024), BF),
            vm((16, 16, 1024), BF), vm((2048, 512), BF), vm((2048, 512), BF), vm((512, 2048), BF),
            vm((32, 2048), BF), vm((16, 128), jnp.int32), vm((8, 128, 128), BF), vm((128, n_tok * 128), BF),
            vm((8, 32, 128), F32), vm((8, 32, 128), F32), vm((8, 32, 1024), BF),
            vm((8, 32, 256), BF), vm((8, 32, 256), BF), vm((128, 512), BF), vm((512, 512), BF), vm((32, 2048), BF), vm((256, 128), BF), vm((64, 256), BF),
            vm((n_tok, 2048), F32), vm((256, 2048), BF), vm((256, 512), BF),
            vm((128, 2, 2048), BF), vm((128, 2, 2048), BF), vm((128, 2, 2048), BF), vm((128, 2, 2048), BF),
            dma((14,)), dma((8,)), dma, dma((4,)), dma((2,)), dma((6,)), dma, dma((2,)), dma, dma,
        ],
        compiler_params=pltpu.CompilerParams(collective_id=0, has_side_effects=True, vmem_limit_bytes=61718528),
        name="layer",
    )(
        tokens, positions.reshape(1, n_tok), mix_gain.reshape(1, -1), ret_gain.reshape(1, -1), ffn_gain.reshape(1, -1),
        routes.T, route_weights.T, state, w_query, w_key, w_value, w_out.T, expert_gate, expert_up, expert_down,
    )


def solution(mesh):
    placed = (
        P("ep", None), P("ep"), P("ep", None, None, None), P(), P(), P(), P(), P(), P(None, "ep"), P(),
        P("ep", None), P("ep", None), P("ep", None, None), P("ep", None, None), P("ep", None, None),
    )
    return jax.shard_map(
        shards, mesh=mesh, in_specs=placed, out_specs=(P("ep", None), P("ep", None, None, None)), check_vma=False
    )
```

```python
import math

import jax
import jax.numpy as jnp
from jax import lax
from jax.experimental import pallas as pl
from jax.experimental.pallas import tpu as pltpu
from jax.sharding import PartitionSpec as P

MESH = pl.DeviceIdType.MESH
EPS = 1e-06
BF = jnp.bfloat16
F32 = jnp.float32
STRIDES = (32, 8, 2)


def hops(d):
    return sum((0, 1, 2, 1)[k] for k in d[:3])


LINES = (
    (0, 0), (2, 2), (2, 1), (3, 2), (1, 1), (3, 3), (1, 0), (0, 3),
    (2, 3), (1, 2), (2, 0), (0, 2), (1, 3), (3, 1), (3, 0), (0, 1),
)
MOVES = [
    sorted(
        [(l, *LINES[l], x, c) for l in range(n * 8, n * 8 + 8) for x in range(4) for c in range(2) if LINES[l] + (x, c) != (0,) * 4],
        key=lambda d: (-hops(d[1:]), d),
    )
    for n in range(2)
]


def kernel(
    tokens_h, pos_h, mixg_h, retg_h, ffng_h, routes_h, rw_h,
    state, wq, wk, wv, wo, eg, eu, ed,
    result, new_state,
    tokens, pos, mixg, retg, ffng, routes_t, rw_t, wqv, wkv, wvv, wh, egv, euv, edv,
    xin, tab, kq, ee, vt, rt, mix, res_out, res_in, tok_out, tok_in, lined, spread, sorted_in, gains, plan, dall, xq, chl, rsd, xs, hid,
    send1, recv1, send2, recv2,
    lsem, ssem_in, ag_s, ag_r, ps, pr, a_s, a_r, b_s, b_r,
):
    me = lax.axis_index("ep")
    co = (me // 32, (me // 8) % 4, (me // 2) % 4)
    c = me % 2
    own = co[0] * 4 + co[1]
    n_tok = tokens.shape[0]

    def along(axis, d):
        return ((co[axis] + d) % 4 - co[axis]) * STRIDES[axis]

    line = [(me + along(0, d), ((co[0] + d) % 4, co[1])) for d in (2, 1, 3)]
    cross = [(me + along(1, d), (co[0], (co[1] + d) % 4)) for d in (2, 1, 3)]

    seat = co[2] * 2 + c
    mates = [(me + along(2, d), (co[2] + d) % 4 * 2 + c) for d in (2, 1, 3)]
    mates.append((me + 1 - 2 * c, seat + 1 - 2 * c))
    others = mates + [(there + 1 - 2 * c, its_seat + 1 - 2 * c) for there, its_seat in mates[:3]]

    bar = pltpu.get_barrier_semaphore()
    for there, _ in others:
        pl.semaphore_signal(bar, inc=1, device_id=(there,), device_id_type=MESH)
    for there, _ in line + cross:
        pl.semaphore_signal(bar, inc=1, device_id=(there,), device_id_type=MESH)

    def fetch(n, src, dst):
        cp = pltpu.make_async_copy(src, dst, lsem.at[n])
        cp.start()
        return cp

    cp_tok = fetch(7, tokens_h, tokens)
    cp_mixg = fetch(8, mixg_h, mixg)
    cp_rt = fetch(9, routes_h, routes_t)
    cp_rw = fetch(10, rw_h, rw_t)
    cp_pos = fetch(11, pos_h, pos)
    cp_wo = fetch(0, wo, wh.at[own])
    cp_k = fetch(1, wk, wkv)
    cp_q = fetch(2, wq, wqv)
    cp_v = fetch(3, wv, wvv)

    def state_in(h):
        return pltpu.make_async_copy(state.at[:, h], new_state.at[:, h], ssem_in.at[h])

    for h in range(4):
        state_in(h).start()
    cp_retg = fetch(12, retg_h, retg)
    cp_ffng = fetch(13, ffng_h, ffng)
    cp_rt.wait()
    cp_rw.wait()
    cp_pos.wait()

    tab[...] = jnp.full(tab.shape, -1, jnp.int32)
    tab[0:6, 0:n_tok] = routes_t[...]
    tab[8:9, 0:n_tok] = pos[...]
    wtab = jnp.concatenate([rw_t[...], jnp.zeros((6, 128 - n_tok), F32)], axis=1)
    rows = lax.broadcasted_iota(jnp.int32, (256, 128), 0)
    expert = rows // 2
    slot = (rows % 2).astype(F32)
    member = jnp.zeros((256, 128), F32)
    weight = jnp.zeros((256, 128), F32)
    for k in range(6):
        hit = tab[k : k + 1, :] == expert
        member = member + jnp.where(hit, 1.0, 0.0)
        weight = weight + jnp.where(hit, wtab[k : k + 1, :], 0.0)
    before = jnp.where(
        lax.broadcasted_iota(jnp.int32, (128, 128), 0) < lax.broadcasted_iota(jnp.int32, (128, 128), 1), 1.0, 0.0
    ).astype(BF)
    place = jnp.dot(member.astype(BF), before, preferred_element_type=F32)
    chosen = jnp.where(place == slot, member, 0.0)
    plan[seat] = jnp.full((8, 128), -1.0, F32)
    plan[seat, 0:6, 0:n_tok] = routes_t[...].astype(F32)
    comb = (chosen * weight).T
    high = comb.astype(BF)
    chl[0:32, :] = high[0:32, :]
    chl[32:64, :] = (comb - high.astype(F32)).astype(BF)[0:32, :]

    erow = lax.broadcasted_iota(jnp.int32, (128, 128), 0)
    etok = jnp.where(erow < 64, erow % 32, -1)
    for t in range(n_tok):
        ee[:, t * 128 : (t + 1) * 128] = jnp.where(etok == t, 1.0, 0.0).astype(BF)

    spots = tab[8:9, 0:32].astype(F32)
    freqs = jnp.exp(-math.log(10000.0) * lax.broadcasted_iota(jnp.int32, (32, 32), 0).astype(F32) / 32.0)
    angle = spots * freqs
    cosine = jnp.cos(angle)
    sine = jnp.sin(angle)

    cp_tok.wait()
    cp_mixg.wait()
    wide = tokens[...].astype(F32)
    scaled = wide * lax.rsqrt(jnp.mean(wide * wide, axis=-1, keepdims=True) + EPS)
    xin[...] = jnp.zeros(xin.shape, BF)
    xin[0:n_tok, :] = (scaled * mixg[...]).astype(BF)

    def send_block(cc, part, peers, sem):
        piece = wh.at[cc[0] * 4 + cc[1], :, pl.ds(part * 512, 512)]
        for there, _ in peers:
            pltpu.make_async_remote_copy(
                src_ref=piece, dst_ref=piece, send_sem=ag_s, recv_sem=ag_r.at[sem],
                device_id=(there,), device_id_type=MESH,
            ).start()

    def gathered(n, sem):
        seen = wh.at[pl.ds(0, n), :, pl.ds(0, 512)]
        pltpu.make_async_copy(seen, seen, ag_r.at[sem]).wait()

    def gather_start():
        here = (co[0], co[1])
        send_block(here, 0, line, 0)
        send_block(here, 1, cross, 1)
        send_block(here, 0, cross, 2)
        send_block(here, 1, line, 3)

    def gather_forward():
        gathered(3, 0)
        for _, cc in line:
            send_block(cc, 0, cross, 2)
        gathered(3, 1)
        for _, cc in cross:
            send_block(cc, 1, line, 3)

    def project(wref, n):
        return jnp.dot(xin[...], wref[:, n * 256 : (n + 1) * 256], preferred_element_type=F32).astype(BF).astype(F32)

    def rotated(offset, wref, scale):
        for n in range(2):
            cols = project(wref, n).T
            for s in range(4):
                a = cols[s * 64 : s * 64 + 32, :]
                b = cols[s * 64 + 32 : s * 64 + 64, :]
                for first, value in ((0, a * cosine - b * sine), (32, b * cosine + a * sine)):
                    value = value * scale
                    high = value.astype(BF)
                    low_part = (value - high.astype(F32)).astype(BF)
                    kq[n * 4 + s, offset + first : offset + first + 32, :] = jnp.concatenate(
                        [high, low_part, jnp.zeros((32, 64), BF)], axis=1
                    )

    cp_k.wait()
    rotated(0, wkv, 0.125)
    pl.semaphore_wait(bar, 13)
    cp_wo.wait()
    gather_start()
    for there, _ in others:
        pltpu.make_async_remote_copy(
            src_ref=plan.at[seat], dst_ref=plan.at[seat], send_sem=ps.at[3], recv_sem=pr.at[7],
            device_id=(there,), device_id_type=MESH,
        ).start()
    for h in range(4, 8):
        state_in(h).start()
    cp_q.wait()
    rotated(64, wqv, 1.0)
    cp_v.wait()
    for n in range(4):
        part = project(wvv, n)
        vt[2 * n] = part[:, 0:128]
        vt[2 * n + 1] = part[:, 128:256]

    def seven(buf, sem):
        seen = buf.at[pl.ds(0, 7), pl.ds(0, 24)]
        pltpu.make_async_copy(seen, seen, sem).wait()

    def two_heads(p):
        for h in (2 * p, 2 * p + 1):
            state_in(h).wait()
        lhs = kq[2 * p : 2 * p + 2].reshape(256, 128)
        for g in range(n_tok // 4):
            wide_kq = jnp.dot(lhs, ee[:, g * 512 : (g + 1) * 512], preferred_element_type=F32)
            for n, h in enumerate((2 * p, 2 * p + 1)):
                decay = 1.0 - 2.0 ** (-2 - h)
                for i in range(4):
                    t = g * 4 + i
                    key = wide_kq[n * 128 : n * 128 + 64, i * 128 : (i + 1) * 128]
                    query = wide_kq[n * 128 + 64 : n * 128 + 128, i * 128 : (i + 1) * 128]
                    new = decay * new_state[t, h] + key * vt[h, t : t + 1, :]
                    new_state[t, h] = new
                    rt[h, t : t + 1, :] = jnp.sum(query * new, axis=0, keepdims=True)
        for h in (2 * p, 2 * p + 1):
            read = rt[h, 0:n_tok, :]
            centred = read - jnp.mean(read, axis=-1, keepdims=True)
            normed = centred * lax.rsqrt(jnp.mean(centred * centred, axis=-1, keepdims=True) + EPS)
            mix[seat, 0:n_tok, h * 128 : (h + 1) * 128] = (normed * retg[:, h * 128 : (h + 1) * 128]).astype(BF)
        piece = mix.at[seat, pl.ds(0, 24), pl.ds(p * 256, 256)]
        for n, (there, _) in enumerate(mates):
            pltpu.make_async_remote_copy(
                src_ref=piece, dst_ref=piece, send_sem=ps.at[0], recv_sem=pr.at[2 + (0, 2, 1, 3)[n]],
                device_id=(there,), device_id_type=MESH,
            ).start()

    cp_retg.wait()
    two_heads(0)
    two_heads(1)
    two_heads(2)
    gather_forward()
    two_heads(3)
    cp_g = fetch(4, eg.at[0], egv)
    cp_u = fetch(5, eu.at[0], euv)
    cp_d = fetch(6, ed.at[0], edv)

    srow = lax.broadcasted_iota(jnp.int32, (1024, 128), 0)
    lane = lax.broadcasted_iota(jnp.int32, (1024, 128), 1)
    target = srow % 128 // 16 * 128 + srow // 128 * 16 + srow % 16
    for n in range(8):
        spread[:, n * 128 : (n + 1) * 128] = jnp.where(lane + n * 128 == target, 1.0, 0.0).astype(BF)

    cp_ffng.wait()
    sorted_in[0:n_tok, :] = tokens[:, 0:1024]
    sorted_in[32 : 32 + n_tok, :] = tokens[:, 1024:2048]
    rows = []
    for n in range(2):
        rest = ffng[:, n * 1024 : (n + 1) * 1024]
        for _ in range(3):
            piece = rest.astype(BF).astype(F32)
            rows.append(piece)
            rest = rest - piece
    rows.append(jnp.zeros((10, 1024), F32))
    sorted_in[64:80, :] = jnp.concatenate(rows, axis=0).astype(BF)
    by_core = lax.dot_general(sorted_in[...], spread[...], (((1,), (1,)), ((), ())), preferred_element_type=F32)
    for g in range(8):
        for n in range(2):
            part = by_core[:, g * 128 : (g + 1) * 128]
            tok_out[g, :, n * 128 : (n + 1) * 128] = part[n * 32 : n * 32 + 32, :].astype(BF)
            at = 64 + 3 * n
            gains[g : g + 1, n * 128 : (n + 1) * 128] = part[at : at + 1, :] + part[at + 1 : at + 2, :] + part[at + 2 : at + 3, :]
    for there, its_seat in others:
        pltpu.make_async_remote_copy(
            src_ref=tok_out.at[its_seat, pl.ds(0, 24)], dst_ref=tok_in.at[seat, pl.ds(0, 24)],
            send_sem=ps.at[2], recv_sem=pr.at[6], device_id=(there,), device_id_type=MESH,
        ).start()
    tok_in[seat] = tok_out[seat]
    for n in (1, 2, 0):
        its_seat = mates[n][1]
        block = mix.at[0, pl.ds(0, 24)]
        pltpu.make_async_copy(block, block, pr.at[2 + n]).wait()
        block = mix.at[its_seat, pl.ds(0, 24)]
        pltpu.make_async_remote_copy(
            src_ref=block, dst_ref=block, send_sem=ps.at[0], recv_sem=pr.at[0],
            device_id=(mates[3][0],), device_id_type=MESH,
        ).start()
    routed = plan.at[pl.ds(0, 7)]
    pltpu.make_async_copy(routed, routed, pr.at[7]).wait()
    ids = jnp.concatenate([plan[g, :, 0:32] for g in range(8)], axis=1)
    mrow = lax.broadcasted_iota(jnp.int32, (256, 256), 0)
    mlane = lax.broadcasted_iota(jnp.int32, (256, 256), 1)
    mine_f = jnp.where(mrow % 16 // 2 == mlane // 32, 1.0, 0.0)
    slot_f = (mrow % 2).astype(F32)
    expert_f = (mrow // 16).astype(F32)
    earlier = jnp.where(mrow < mlane, 1.0, 0.0).astype(BF)
    for b in range(8):
        member = jnp.zeros((256, 256), F32)
        shifted_ids = ids - 16.0 * b
        for k in range(6):
            member = jnp.where(shifted_ids[k : k + 1, :] == expert_f, mine_f, member)
        place = jnp.dot(member.astype(BF), earlier, preferred_element_type=F32)
        dall[b * 256 : (b + 1) * 256, :] = jnp.where(place == slot_f, member, 0.0).astype(BF)
    gathered(12, 2)
    gathered(12, 3)
    block = mix.at[0, pl.ds(0, 24)]
    pltpu.make_async_copy(block, block, pr.at[5]).wait()
    pltpu.make_async_copy(mix.at[pl.ds(0, 3), pl.ds(0, 24)], mix.at[pl.ds(0, 3), pl.ds(0, 24)], pr.at[0]).wait()
    seven(tok_in, pr.at[6])
    attended = lax.dot_general(
        mix[...].reshape(256, 1024), wh[...].reshape(256, 1024), (((1,), (1,)), ((), ())), preferred_element_type=F32
    ).astype(BF).astype(F32)
    piece = (tok_in[...].reshape(256, 256).astype(F32) + attended).astype(BF).astype(F32)
    real = lax.broadcasted_iota(jnp.int32, (256, 256), 0) % 32 < n_tok
    piece = jnp.where(real, piece, 0.0).astype(BF)
    res_out[...] = piece.reshape(8, 32, 256)
    for b in range(8):
        out = jnp.dot(dall[b * 256 : (b + 1) * 256, :], piece, preferred_element_type=F32)
        send1[b * 16 : (b + 1) * 16] = out.astype(BF).reshape(16, 16, 256)

    def peers(half, sign, put):
        zs = [(co[0] + sign * d) % 4 * 32 for d in range(4)]
        ys = [(co[1] + sign * d) % 4 * 8 for d in range(4)]
        xs4 = [(co[2] + sign * d) % 4 * 2 for d in range(4)]
        cs = [c, 1 - c]
        for l, dz, dy, dx, dc in MOVES[half]:
            its_seat = xs4[dx] + cs[dc]
            put(l, its_seat, zs[dz] + ys[dy] + its_seat)

    def dispatch(half):
        def put(l, its_seat, t):
            pltpu.make_async_remote_copy(
                src_ref=send1.at[t], dst_ref=recv1.at[seat, pl.ds(l * 16, 16)], send_sem=a_s, recv_sem=a_r.at[half],
                device_id=(t,), device_id_type=MESH,
            ).start()

        peers(half, 1, put)

    def give_back(half):
        def put(l, its_seat, t):
            pltpu.make_async_remote_copy(
                src_ref=send2.at[l * 8 + its_seat], dst_ref=recv2.at[me], send_sem=b_s, recv_sem=b_r,
                device_id=(t,), device_id_type=MESH,
            ).start()

        peers(half, -1, put)

    def arrived(buf, first, count, sem):
        seen = buf.at[pl.ds(first, count)]
        pltpu.make_async_copy(seen, seen, sem).wait()

    def experts(half):
        mine = slice(half * 128, half * 128 + 128)
        square = jnp.zeros((128, 128), F32)
        for g in range(8):
            value = recv1[g, mine, :].astype(F32)
            value = value * value
            square = square + value[:, 0:128] + value[:, 128:256]
        inv = lax.rsqrt(jnp.sum(square, axis=-1, keepdims=True) / 2048.0 + EPS)
        for g in range(8):
            xq[g] = (recv1[g, mine, :].astype(F32) * inv * gains[g : g + 1, :]).astype(BF)

        def rows_of(ref, g, cols):
            return jnp.concatenate([ref[n * 128 + g * 16 : n * 128 + g * 16 + 16, cols] for n in range(16)], axis=0)

        for n in range(2):
            cols = slice(n * 256, (n + 1) * 256)
            gate = jnp.zeros((128, 256), F32)
            up = jnp.zeros((128, 256), F32)
            for g in range(8):
                gate = gate + jnp.dot(xq[g], rows_of(egv, g, cols), preferred_element_type=F32)
                up = up + jnp.dot(xq[g], rows_of(euv, g, cols), preferred_element_type=F32)
            hid[mine, cols] = (jax.nn.silu(gate) * up).astype(BF)
        for n in range(8):
            cols = slice(n * 256, (n + 1) * 256)
            out = jnp.dot(hid[mine, :], edv[:, cols], preferred_element_type=F32).astype(BF)
            send2[half * 64 : half * 64 + 64, :, cols] = out.reshape(64, 2, 256)

    dispatch(0)
    dispatch(1)
    recv1[seat, 0:16, :] = send1[me]
    for there, its_seat in others:
        pltpu.make_async_remote_copy(
            src_ref=res_out.at[its_seat, pl.ds(0, 24)], dst_ref=res_in.at[seat, pl.ds(0, 24)],
            send_sem=ps.at[1], recv_sem=pr.at[1], device_id=(there,), device_id_type=MESH,
        ).start()
    res_in[seat] = res_out[seat]
    cp_g.wait()
    cp_u.wait()
    cp_d.wait()
    arrived(send1, 0, 63, a_r.at[0])
    experts(0)
    give_back(0)
    recv2[me] = send2[seat]
    arrived(send1, 0, 64, a_r.at[1])
    experts(1)
    give_back(1)
    seven(res_in, pr.at[1])
    for n in range(2):
        for g in range(8):
            lined[n * 32 : (n + 1) * 32, g * 128 : (g + 1) * 128] = res_in[g, :, n * 128 : (n + 1) * 128]
    resid = jnp.dot(lined[...], spread[...], preferred_element_type=F32)
    rsd[:, 0:1024] = resid[0:n_tok, :]
    rsd[:, 1024:2048] = resid[32 : 32 + n_tok, :]
    arrived(recv2, 0, 127, b_r)

    def unpack2(i, _):
        xs[pl.ds(i * 16, 16), :] = recv2[pl.ds(i * 8, 8)].reshape(16, 2048)
        return 0

    lax.fori_loop(0, 16, unpack2, 0)
    for n in range(8):
        cols = slice(n * 256, (n + 1) * 256)
        got = jnp.dot(chl[...], xs[:, cols], preferred_element_type=F32)
        result[:, cols] = (rsd[:, cols] + got[0:n_tok, :] + got[32 : 32 + n_tok, :]).astype(BF)

    arrived(send1, 0, 127, a_s)
    arrived(send2, 0, 127, b_s)
    sent = wh.at[pl.ds(0, 15)]
    pltpu.make_async_copy(sent, sent, ag_s).wait()
    seven(mix, ps.at[0])
    seven(res_out, ps.at[1])
    seven(tok_out, ps.at[2])
    pltpu.make_async_copy(routed, routed, ps.at[3]).wait()


def hand_over(result, new_state, result_out, state_out, sems):
    copies = [pltpu.make_async_copy(result, result_out, sems.at[10])]
    for n in range(10):
        rows = pl.ds(n * 2, 2)
        copies.append(pltpu.make_async_copy(new_state.at[rows], state_out.at[rows], sems.at[n]))
    for cp in copies:
        cp.start()
    for cp in copies:
        cp.wait()


def shards(
    tokens, positions, state, mix_gain, w_query, w_key, w_value, ret_gain, w_out, ffn_gain,
    routes, route_weights, expert_gate, expert_up, expert_down,
):
    vmem = pl.BlockSpec(memory_space=pltpu.VMEM)
    hbm = pl.BlockSpec(memory_space=pl.ANY)
    n_tok = tokens.shape[0]
    dma = pltpu.SemaphoreType.DMA
    vm = pltpu.VMEM
    result, new_state = pl.pallas_call(
        kernel,
        out_shape=(
            pltpu.VMEM(tokens.shape, BF),
            pltpu.VMEM(state.shape, F32),
        ),
        in_specs=[hbm] * 15,
        out_specs=(vmem, vmem),
        scratch_shapes=[
            vm((n_tok, 2048), BF), vm((1, n_tok), jnp.int32), vm((1, 2048), F32), vm((1, 1024), F32), vm((1, 2048), F32),
            vm((6, n_tok), jnp.int32), vm((6, n_tok), F32),
            vm((2048, 512), BF), vm((2048, 512), BF), vm((2048, 1024), BF),
            vm((16, 16, 1024), BF), vm((2048, 512), BF), vm((2048, 512), BF), vm((512, 2048), BF),
            vm((32, 2048), BF), vm((16, 128), jnp.int32), vm((8, 128, 128), BF), vm((128, n_tok * 128), BF),
            vm((8, 32, 128), F32), vm((8, 32, 128), F32), vm((8, 32, 1024), BF),
            vm((8, 32, 256), BF), vm((8, 32, 256), BF), vm((8, 32, 256), BF), vm((8, 32, 256), BF),
            vm((64, 1024), BF), vm((1024, 1024), BF), vm((80, 1024), BF), vm((8, 256), F32), vm((8, 8, 128), F32),
            vm((2048, 256), BF), vm((8, 128, 256), BF), vm((64, 256), BF),
            vm((n_tok, 2048), F32), vm((256, 2048), BF), vm((256, 512), BF),
            vm((128, 16, 256), BF), vm((8, 256, 256), BF), vm((128, 2, 2048), BF), vm((128, 2, 2048), BF),
            dma((14,)), dma((8,)), dma, dma((4,)), dma((4,)), dma((8,)), dma, dma((2,)), dma, dma,
        ],
        compiler_params=pltpu.CompilerParams(collective_id=0, has_side_effects=True, vmem_limit_bytes=61650000),
        name="layer",
    )(
        tokens, positions.reshape(1, n_tok), mix_gain.reshape(1, -1), ret_gain.reshape(1, -1), ffn_gain.reshape(1, -1),
        routes.T, route_weights.T, state, w_query, w_key, w_value, w_out.T, expert_gate, expert_up, expert_down,
    )
    return pl.pallas_call(
        hand_over,
        out_shape=(jax.ShapeDtypeStruct(tokens.shape, BF), jax.ShapeDtypeStruct(state.shape, F32)),
        in_specs=[vmem] * 2,
        out_specs=(hbm, hbm),
        scratch_shapes=[dma((11,))],
        compiler_params=pltpu.CompilerParams(vmem_limit_bytes=1 << 20),
        name="hand_over",
    )(result, new_state)


def solution(mesh):
    placed = (
        P("ep", None), P("ep"), P("ep", None, None, None), P(), P(), P(), P(), P(), P(None, "ep"), P(),
        P("ep", None), P("ep", None), P("ep", None, None), P("ep", None, None), P("ep", None, None),
    )
    return jax.shard_map(
        shards, mesh=mesh, in_specs=placed, out_specs=(P("ep", None), P("ep", None, None, None)), check_vma=False
    )
```

```python
import math

import jax
import jax.numpy as jnp
from jax import lax
from jax.experimental import pallas as pl
from jax.experimental.pallas import tpu as pltpu
from jax.sharding import PartitionSpec as P

MESH = pl.DeviceIdType.MESH
EPS = 1e-06
BF = jnp.bfloat16
F32 = jnp.float32
STRIDES = (32, 8, 2)


def hops(d):
    return sum((0, 1, 2, 1)[k] for k in d[:3])


LINES = (
    (0, 0), (2, 2), (2, 1), (3, 2), (1, 1), (3, 3), (1, 0), (0, 3),
    (2, 3), (1, 2), (2, 0), (0, 2), (1, 3), (3, 1), (3, 0), (0, 1),
)
BOUNDS = (0, 8, 16)
MOVES = [
    sorted(
        [(l, *LINES[l], x, c) for l in range(a, b) for x in range(4) for c in range(2) if LINES[l] + (x, c) != (0,) * 4],
        key=lambda d: (-hops(d[1:]), d[3], -d[0], d[4]),
    )
    for a, b in zip(BOUNDS[:-1], BOUNDS[1:])
]


def kernel(
    tokens_h, pos_h, mixg_h, retg_h, ffng_h, routes_h, rw_h,
    state, wq, wk, wv, wo, eg, eu, ed,
    result, new_state,
    tokens, pos, mixg, retg, ffng, routes_t, rw_t, wqv, wkv, wvv, wh, egv, euv, edv,
    xin, tab, kq, ee, vt, rt, mix, res_out, res_in, tok_out, tok_in, lined, spread, sorted_in, gains, plan, dall, xq, chl, rsd, xs, hid,
    send1, recv1, send2, recv2,
    lsem, ssem_in, ag_s, ag_r, ps, pr, a_s, a_r, b_s, b_r,
):
    me = lax.axis_index("ep")
    co = (me // 32, (me // 8) % 4, (me // 2) % 4)
    c = me % 2
    own = co[0] * 4 + co[1]
    n_tok = tokens.shape[0]

    def along(axis, d):
        return ((co[axis] + d) % 4 - co[axis]) * STRIDES[axis]

    line = [(me + along(0, d), ((co[0] + d) % 4, co[1])) for d in (2, 1, 3)]
    cross = [(me + along(1, d), (co[0], (co[1] + d) % 4)) for d in (2, 1, 3)]

    seat = co[2] * 2 + c
    mates = [(me + along(2, d), (co[2] + d) % 4 * 2 + c) for d in (2, 1, 3)]
    mates.append((me + 1 - 2 * c, seat + 1 - 2 * c))
    others = mates + [(there + 1 - 2 * c, its_seat + 1 - 2 * c) for there, its_seat in mates[:3]]

    bar = pltpu.get_barrier_semaphore()
    for there, _ in others:
        pl.semaphore_signal(bar, inc=1, device_id=(there,), device_id_type=MESH)
    for there, _ in line + cross:
        pl.semaphore_signal(bar, inc=1, device_id=(there,), device_id_type=MESH)

    def fetch(n, src, dst):
        cp = pltpu.make_async_copy(src, dst, lsem.at[n])
        cp.start()
        return cp

    cp_tok = fetch(7, tokens_h, tokens)
    cp_mixg = fetch(8, mixg_h, mixg)
    cp_rt = fetch(9, routes_h, routes_t)
    cp_rw = fetch(10, rw_h, rw_t)
    cp_pos = fetch(11, pos_h, pos)
    cp_wo = fetch(0, wo, wh.at[own])
    cp_k = fetch(1, wk, wkv)
    cp_q = fetch(2, wq, wqv)
    cp_v = fetch(3, wv, wvv)

    def state_in(h):
        return pltpu.make_async_copy(state.at[:, h], new_state.at[:, h], ssem_in.at[h])

    for h in range(4):
        state_in(h).start()
    cp_retg = fetch(12, retg_h, retg)
    cp_ffng = fetch(13, ffng_h, ffng)
    cp_rt.wait()
    cp_rw.wait()
    cp_pos.wait()

    tab[...] = jnp.full(tab.shape, -1, jnp.int32)
    tab[0:6, 0:n_tok] = routes_t[...]
    tab[8:9, 0:n_tok] = pos[...]
    wtab = jnp.concatenate([rw_t[...], jnp.zeros((6, 128 - n_tok), F32)], axis=1)
    rows = lax.broadcasted_iota(jnp.int32, (256, 128), 0)
    expert = rows // 2
    slot = (rows % 2).astype(F32)
    member = jnp.zeros((256, 128), F32)
    weight = jnp.zeros((256, 128), F32)
    for k in range(6):
        hit = tab[k : k + 1, :] == expert
        member = member + jnp.where(hit, 1.0, 0.0)
        weight = weight + jnp.where(hit, wtab[k : k + 1, :], 0.0)
    before = jnp.where(
        lax.broadcasted_iota(jnp.int32, (128, 128), 0) < lax.broadcasted_iota(jnp.int32, (128, 128), 1), 1.0, 0.0
    ).astype(BF)
    place = jnp.dot(member.astype(BF), before, preferred_element_type=F32)
    chosen = jnp.where(place == slot, member, 0.0)
    plan[seat] = jnp.full((8, 128), -1.0, F32)
    plan[seat, 0:6, 0:n_tok] = routes_t[...].astype(F32)
    comb = (chosen * weight).T
    high = comb.astype(BF)
    chl[0:32, :] = high[0:32, :]
    chl[32:64, :] = (comb - high.astype(F32)).astype(BF)[0:32, :]

    erow = lax.broadcasted_iota(jnp.int32, (128, 128), 0)
    etok = jnp.where(erow < 64, erow % 32, -1)
    for t in range(n_tok):
        ee[:, t * 128 : (t + 1) * 128] = jnp.where(etok == t, 1.0, 0.0).astype(BF)

    spots = tab[8:9, 0:32].astype(F32)
    freqs = jnp.exp(-math.log(10000.0) * lax.broadcasted_iota(jnp.int32, (32, 32), 0).astype(F32) / 32.0)
    angle = spots * freqs
    cosine = jnp.cos(angle)
    sine = jnp.sin(angle)

    cp_tok.wait()
    cp_mixg.wait()
    wide = tokens[...].astype(F32)
    scaled = wide * lax.rsqrt(jnp.mean(wide * wide, axis=-1, keepdims=True) + EPS)
    xin[...] = jnp.zeros(xin.shape, BF)
    xin[0:n_tok, :] = (scaled * mixg[...]).astype(BF)

    def send_block(cc, part, peers, sem):
        piece = wh.at[cc[0] * 4 + cc[1], :, pl.ds(part * 512, 512)]
        for there, _ in peers:
            pltpu.make_async_remote_copy(
                src_ref=piece, dst_ref=piece, send_sem=ag_s, recv_sem=ag_r.at[sem],
                device_id=(there,), device_id_type=MESH,
            ).start()

    def gathered(n, sem):
        seen = wh.at[pl.ds(0, n), :, pl.ds(0, 512)]
        pltpu.make_async_copy(seen, seen, ag_r.at[sem]).wait()

    def gather_start():
        here = (co[0], co[1])
        send_block(here, 0, line, 0)
        send_block(here, 1, cross, 1)
        send_block(here, 0, cross, 2)
        send_block(here, 1, line, 3)

    def gather_forward():
        gathered(3, 0)
        for _, cc in line:
            send_block(cc, 0, cross, 2)
        gathered(3, 1)
        for _, cc in cross:
            send_block(cc, 1, line, 3)

    def project(wref, n):
        return jnp.dot(xin[...], wref[:, n * 256 : (n + 1) * 256], preferred_element_type=F32).astype(BF).astype(F32)

    def rotated(offset, wref, scale):
        for n in range(2):
            cols = project(wref, n).T
            for s in range(4):
                a = cols[s * 64 : s * 64 + 32, :]
                b = cols[s * 64 + 32 : s * 64 + 64, :]
                for first, value in ((0, a * cosine - b * sine), (32, b * cosine + a * sine)):
                    value = value * scale
                    high = value.astype(BF)
                    low_part = (value - high.astype(F32)).astype(BF)
                    kq[n * 4 + s, offset + first : offset + first + 32, :] = jnp.concatenate(
                        [high, low_part, jnp.zeros((32, 64), BF)], axis=1
                    )

    cp_k.wait()
    rotated(0, wkv, 0.125)
    pl.semaphore_wait(bar, 13)
    cp_wo.wait()
    gather_start()
    for there, _ in others:
        pltpu.make_async_remote_copy(
            src_ref=plan.at[seat], dst_ref=plan.at[seat], send_sem=ps.at[3], recv_sem=pr.at[7],
            device_id=(there,), device_id_type=MESH,
        ).start()
    for h in range(4, 8):
        state_in(h).start()
    cp_q.wait()
    rotated(64, wqv, 1.0)
    cp_v.wait()
    for n in range(4):
        part = project(wvv, n)
        vt[2 * n] = part[:, 0:128]
        vt[2 * n + 1] = part[:, 128:256]

    def seven(buf, sem):
        seen = buf.at[pl.ds(0, 7), pl.ds(0, 24)]
        pltpu.make_async_copy(seen, seen, sem).wait()

    def two_heads(p):
        for h in (2 * p, 2 * p + 1):
            state_in(h).wait()
        lhs = kq[2 * p : 2 * p + 2].reshape(256, 128)
        for g in range(n_tok // 4):
            wide_kq = jnp.dot(lhs, ee[:, g * 512 : (g + 1) * 512], preferred_element_type=F32)
            for n, h in enumerate((2 * p, 2 * p + 1)):
                decay = 1.0 - 2.0 ** (-2 - h)
                for i in range(4):
                    t = g * 4 + i
                    key = wide_kq[n * 128 : n * 128 + 64, i * 128 : (i + 1) * 128]
                    query = wide_kq[n * 128 + 64 : n * 128 + 128, i * 128 : (i + 1) * 128]
                    new = decay * new_state[t, h] + key * vt[h, t : t + 1, :]
                    new_state[t, h] = new
                    rt[h, t : t + 1, :] = jnp.sum(query * new, axis=0, keepdims=True)
        for h in (2 * p, 2 * p + 1):
            read = rt[h, 0:n_tok, :]
            centred = read - jnp.mean(read, axis=-1, keepdims=True)
            normed = centred * lax.rsqrt(jnp.mean(centred * centred, axis=-1, keepdims=True) + EPS)
            mix[seat, 0:n_tok, h * 128 : (h + 1) * 128] = (normed * retg[:, h * 128 : (h + 1) * 128]).astype(BF)
        piece = mix.at[seat, pl.ds(0, 24), pl.ds(p * 256, 256)]
        for n, (there, _) in enumerate(mates):
            pltpu.make_async_remote_copy(
                src_ref=piece, dst_ref=piece, send_sem=ps.at[0], recv_sem=pr.at[2 + (0, 2, 1, 3)[n]],
                device_id=(there,), device_id_type=MESH,
            ).start()

    cp_retg.wait()
    two_heads(0)
    two_heads(1)
    two_heads(2)
    gather_forward()
    two_heads(3)
    cp_g = fetch(4, eg.at[0], egv)
    cp_u = fetch(5, eu.at[0], euv)
    cp_d = fetch(6, ed.at[0], edv)

    srow = lax.broadcasted_iota(jnp.int32, (1024, 128), 0)
    lane = lax.broadcasted_iota(jnp.int32, (1024, 128), 1)
    target = srow % 128 // 16 * 128 + srow // 128 * 16 + srow % 16
    for n in range(8):
        spread[:, n * 128 : (n + 1) * 128] = jnp.where(lane + n * 128 == target, 1.0, 0.0).astype(BF)

    cp_ffng.wait()
    sorted_in[0:n_tok, :] = tokens[:, 0:1024]
    sorted_in[32 : 32 + n_tok, :] = tokens[:, 1024:2048]
    rows = []
    for n in range(2):
        rest = ffng[:, n * 1024 : (n + 1) * 1024]
        for _ in range(3):
            piece = rest.astype(BF).astype(F32)
            rows.append(piece)
            rest = rest - piece
    rows.append(jnp.zeros((10, 1024), F32))
    sorted_in[64:80, :] = jnp.concatenate(rows, axis=0).astype(BF)
    by_core = lax.dot_general(sorted_in[...], spread[...], (((1,), (1,)), ((), ())), preferred_element_type=F32)
    for g in range(8):
        for n in range(2):
            part = by_core[:, g * 128 : (g + 1) * 128]
            tok_out[g, :, n * 128 : (n + 1) * 128] = part[n * 32 : n * 32 + 32, :].astype(BF)
            at = 64 + 3 * n
            gains[g : g + 1, n * 128 : (n + 1) * 128] = part[at : at + 1, :] + part[at + 1 : at + 2, :] + part[at + 2 : at + 3, :]
    for there, its_seat in others:
        pltpu.make_async_remote_copy(
            src_ref=tok_out.at[its_seat, pl.ds(0, 24)], dst_ref=tok_in.at[seat, pl.ds(0, 24)],
            send_sem=ps.at[2], recv_sem=pr.at[6], device_id=(there,), device_id_type=MESH,
        ).start()
    tok_in[seat] = tok_out[seat]
    for n in (1, 2, 0):
        its_seat = mates[n][1]
        block = mix.at[0, pl.ds(0, 24)]
        pltpu.make_async_copy(block, block, pr.at[2 + n]).wait()
        block = mix.at[its_seat, pl.ds(0, 24)]
        pltpu.make_async_remote_copy(
            src_ref=block, dst_ref=block, send_sem=ps.at[0], recv_sem=pr.at[0],
            device_id=(mates[3][0],), device_id_type=MESH,
        ).start()
    routed = plan.at[pl.ds(0, 7)]
    pltpu.make_async_copy(routed, routed, pr.at[7]).wait()
    ids = jnp.concatenate([plan[g, :, 0:32] for g in range(8)], axis=1)
    mrow = lax.broadcasted_iota(jnp.int32, (256, 256), 0)
    mlane = lax.broadcasted_iota(jnp.int32, (256, 256), 1)
    mine_f = jnp.where(mrow % 16 // 2 == mlane // 32, 1.0, 0.0)
    slot_f = (mrow % 2).astype(F32)
    expert_f = (mrow // 16).astype(F32)
    earlier = jnp.where(mrow < mlane, 1.0, 0.0).astype(BF)
    for b in range(8):
        member = jnp.zeros((256, 256), F32)
        shifted_ids = ids - 16.0 * b
        for k in range(6):
            member = jnp.where(shifted_ids[k : k + 1, :] == expert_f, mine_f, member)
        place = jnp.dot(member.astype(BF), earlier, preferred_element_type=F32)
        dall[b * 256 : (b + 1) * 256, :] = jnp.where(place == slot_f, member, 0.0).astype(BF)
    gathered(12, 2)
    gathered(12, 3)
    block = mix.at[0, pl.ds(0, 24)]
    pltpu.make_async_copy(block, block, pr.at[5]).wait()
    pltpu.make_async_copy(mix.at[pl.ds(0, 3), pl.ds(0, 24)], mix.at[pl.ds(0, 3), pl.ds(0, 24)], pr.at[0]).wait()
    seven(tok_in, pr.at[6])
    attended = lax.dot_general(
        mix[...].reshape(256, 1024), wh[...].reshape(256, 1024), (((1,), (1,)), ((), ())), preferred_element_type=F32
    ).astype(BF).astype(F32)
    piece = (tok_in[...].reshape(256, 256).astype(F32) + attended).astype(BF).astype(F32)
    real = lax.broadcasted_iota(jnp.int32, (256, 256), 0) % 32 < n_tok
    piece = jnp.where(real, piece, 0.0).astype(BF)
    res_out[...] = piece.reshape(8, 32, 256)
    for b in range(8):
        out = jnp.dot(dall[b * 256 : (b + 1) * 256, :], piece, preferred_element_type=F32)
        send1[b * 16 : (b + 1) * 16] = out.astype(BF).reshape(16, 16, 256)

    def peers(half, sign, put):
        zs = [(co[0] + sign * d) % 4 * 32 for d in range(4)]
        ys = [(co[1] + sign * d) % 4 * 8 for d in range(4)]
        xs4 = [(co[2] + sign * d) % 4 * 2 for d in range(4)]
        cs = [c, 1 - c]
        for l, dz, dy, dx, dc in MOVES[half]:
            its_seat = xs4[dx] + cs[dc]
            put(l, its_seat, zs[dz] + ys[dy] + its_seat)

    def dispatch(half):
        def put(l, its_seat, t):
            pltpu.make_async_remote_copy(
                src_ref=send1.at[t], dst_ref=recv1.at[seat, pl.ds(l * 16, 16)], send_sem=a_s, recv_sem=a_r.at[half],
                device_id=(t,), device_id_type=MESH,
            ).start()

        peers(half, 1, put)

    def give_back(half):
        def put(l, its_seat, t):
            pltpu.make_async_remote_copy(
                src_ref=send2.at[l * 8 + its_seat], dst_ref=recv2.at[me], send_sem=b_s, recv_sem=b_r,
                device_id=(t,), device_id_type=MESH,
            ).start()

        peers(half, -1, put)

    def arrived(buf, first, count, sem):
        seen = buf.at[pl.ds(first, count)]
        pltpu.make_async_copy(seen, seen, sem).wait()

    def experts(half):
        first, n_rows = BOUNDS[half] * 16, (BOUNDS[half + 1] - BOUNDS[half]) * 16
        mine = slice(first, first + n_rows)
        square = jnp.zeros((n_rows, 128), F32)
        for g in range(8):
            value = recv1[g, mine, :].astype(F32)
            value = value * value
            square = square + value[:, 0:128] + value[:, 128:256]
        inv = lax.rsqrt(jnp.sum(square, axis=-1, keepdims=True) / 2048.0 + EPS)
        for g in range(8):
            xq[g, 0:n_rows, :] = (recv1[g, mine, :].astype(F32) * inv * gains[g : g + 1, :]).astype(BF)

        def rows_of(ref, g, cols):
            return jnp.concatenate([ref[n * 128 + g * 16 : n * 128 + g * 16 + 16, cols] for n in range(16)], axis=0)

        for n in range(2):
            cols = slice(n * 256, (n + 1) * 256)
            gate = jnp.zeros((n_rows, 256), F32)
            up = jnp.zeros((n_rows, 256), F32)
            for g in range(8):
                gate = gate + jnp.dot(xq[g, 0:n_rows, :], rows_of(egv, g, cols), preferred_element_type=F32)
                up = up + jnp.dot(xq[g, 0:n_rows, :], rows_of(euv, g, cols), preferred_element_type=F32)
            hid[mine, cols] = (jax.nn.silu(gate) * up).astype(BF)
        for n in range(8):
            cols = slice(n * 256, (n + 1) * 256)
            out = jnp.dot(hid[mine, :], edv[:, cols], preferred_element_type=F32).astype(BF)
            send2[first // 2 : (first + n_rows) // 2, :, cols] = out.reshape(n_rows // 2, 2, 256)

    for n in range(len(MOVES)):
        dispatch(n)
    recv1[seat, 0:16, :] = send1[me]
    for there, its_seat in others:
        pltpu.make_async_remote_copy(
            src_ref=res_out.at[its_seat, pl.ds(0, 24)], dst_ref=res_in.at[seat, pl.ds(0, 24)],
            send_sem=ps.at[1], recv_sem=pr.at[1], device_id=(there,), device_id_type=MESH,
        ).start()
    res_in[seat] = res_out[seat]
    cp_g.wait()
    cp_u.wait()
    cp_d.wait()
    arrived(send1, 0, 63, a_r.at[0])
    experts(0)
    give_back(0)
    recv2[me] = send2[seat]
    arrived(send1, 0, 64, a_r.at[1])
    experts(1)
    give_back(1)
    seven(res_in, pr.at[1])
    for n in range(2):
        for g in range(8):
            lined[n * 32 : (n + 1) * 32, g * 128 : (g + 1) * 128] = res_in[g, :, n * 128 : (n + 1) * 128]
    resid = jnp.dot(lined[...], spread[...], preferred_element_type=F32)
    rsd[:, 0:1024] = resid[0:n_tok, :]
    rsd[:, 1024:2048] = resid[32 : 32 + n_tok, :]
    arrived(recv2, 0, 127, b_r)

    def unpack2(i, _):
        xs[pl.ds(i * 16, 16), :] = recv2[pl.ds(i * 8, 8)].reshape(16, 2048)
        return 0

    lax.fori_loop(0, 16, unpack2, 0)
    for n in range(8):
        cols = slice(n * 256, (n + 1) * 256)
        got = jnp.dot(chl[...], xs[:, cols], preferred_element_type=F32)
        result[:, cols] = (rsd[:, cols] + got[0:n_tok, :] + got[32 : 32 + n_tok, :]).astype(BF)

    arrived(send1, 0, 127, a_s)
    arrived(send2, 0, 127, b_s)
    sent = wh.at[pl.ds(0, 15)]
    pltpu.make_async_copy(sent, sent, ag_s).wait()
    seven(mix, ps.at[0])
    seven(res_out, ps.at[1])
    seven(tok_out, ps.at[2])
    pltpu.make_async_copy(routed, routed, ps.at[3]).wait()


def hand_over(result, new_state, result_out, state_out, sems):
    copies = [pltpu.make_async_copy(result, result_out, sems.at[10])]
    for n in range(10):
        rows = pl.ds(n * 2, 2)
        copies.append(pltpu.make_async_copy(new_state.at[rows], state_out.at[rows], sems.at[n]))
    for cp in copies:
        cp.start()
    for cp in copies:
        cp.wait()


def shards(
    tokens, positions, state, mix_gain, w_query, w_key, w_value, ret_gain, w_out, ffn_gain,
    routes, route_weights, expert_gate, expert_up, expert_down,
):
    vmem = pl.BlockSpec(memory_space=pltpu.VMEM)
    hbm = pl.BlockSpec(memory_space=pl.ANY)
    n_tok = tokens.shape[0]
    dma = pltpu.SemaphoreType.DMA
    vm = pltpu.VMEM
    result, new_state = pl.pallas_call(
        kernel,
        out_shape=(
            pltpu.VMEM(tokens.shape, BF),
            pltpu.VMEM(state.shape, F32),
        ),
        in_specs=[hbm] * 15,
        out_specs=(vmem, vmem),
        scratch_shapes=[
            vm((n_tok, 2048), BF), vm((1, n_tok), jnp.int32), vm((1, 2048), F32), vm((1, 1024), F32), vm((1, 2048), F32),
            vm((6, n_tok), jnp.int32), vm((6, n_tok), F32),
            vm((2048, 512), BF), vm((2048, 512), BF), vm((2048, 1024), BF),
            vm((16, 16, 1024), BF), vm((2048, 512), BF), vm((2048, 512), BF), vm((512, 2048), BF),
            vm((32, 2048), BF), vm((16, 128), jnp.int32), vm((8, 128, 128), BF), vm((128, n_tok * 128), BF),
            vm((8, 32, 128), F32), vm((8, 32, 128), F32), vm((8, 32, 1024), BF),
            vm((8, 32, 256), BF), vm((8, 32, 256), BF), vm((8, 32, 256), BF), vm((8, 32, 256), BF),
            vm((64, 1024), BF), vm((1024, 1024), BF), vm((80, 1024), BF), vm((8, 256), F32), vm((8, 8, 128), F32),
            vm((2048, 256), BF), vm((8, 128, 256), BF), vm((64, 256), BF),
            vm((n_tok, 2048), F32), vm((256, 2048), BF), vm((256, 512), BF),
            vm((128, 16, 256), BF), vm((8, 256, 256), BF), vm((128, 2, 2048), BF), vm((128, 2, 2048), BF),
            dma((14,)), dma((8,)), dma, dma((4,)), dma((4,)), dma((8,)), dma, dma((2,)), dma, dma,
        ],
        compiler_params=pltpu.CompilerParams(collective_id=0, has_side_effects=True, vmem_limit_bytes=61650000),
        name="layer",
    )(
        tokens, positions.reshape(1, n_tok), mix_gain.reshape(1, -1), ret_gain.reshape(1, -1), ffn_gain.reshape(1, -1),
        routes.T, route_weights.T, state, w_query, w_key, w_value, w_out.T, expert_gate, expert_up, expert_down,
    )
    return pl.pallas_call(
        hand_over,
        out_shape=(jax.ShapeDtypeStruct(tokens.shape, BF), jax.ShapeDtypeStruct(state.shape, F32)),
        in_specs=[vmem] * 2,
        out_specs=(hbm, hbm),
        scratch_shapes=[dma((11,))],
        compiler_params=pltpu.CompilerParams(vmem_limit_bytes=1 << 20),
        name="hand_over",
    )(result, new_state)


def solution(mesh):
    placed = (
        P("ep", None), P("ep"), P("ep", None, None, None), P(), P(), P(), P(), P(), P(None, "ep"), P(),
        P("ep", None), P("ep", None), P("ep", None, None), P("ep", None, None), P("ep", None, None),
    )
    return jax.shard_map(
        shards, mesh=mesh, in_specs=placed, out_specs=(P("ep", None), P("ep", None, None, None)), check_vma=False
    )
```

```python
import math

import jax
import jax.numpy as jnp
from jax import lax
from jax.experimental import pallas as pl
from jax.experimental.pallas import tpu as pltpu
from jax.sharding import PartitionSpec as P

MESH = pl.DeviceIdType.MESH
EPS = 1e-06
BF = jnp.bfloat16
F32 = jnp.float32
STRIDES = (32, 8, 2)


def hops(d):
    return sum((0, 1, 2, 1)[k] for k in d[:3])


LINES = (
    (0, 0), (2, 2), (2, 1), (3, 2), (1, 1), (3, 3), (1, 0), (0, 3),
    (2, 3), (1, 2), (2, 0), (0, 2), (1, 3), (3, 1), (3, 0), (0, 1),
)
BOUNDS = (0, 8, 16)
MOVES = [
    sorted(
        [(l, *LINES[l], x, c) for l in range(a, b) for x in range(4) for c in range(2) if LINES[l] + (x, c) != (0,) * 4],
        key=lambda d: (-hops(d[1:]), d[4], d[3], d[0]),
    )
    for a, b in zip(BOUNDS[:-1], BOUNDS[1:])
]


def kernel(
    tokens_h, pos_h, mixg_h, retg_h, ffng_h, routes_h, rw_h,
    state, wq, wk, wv, wo, eg, eu, ed,
    result, new_state,
    tokens, pos, mixg, retg, ffng, routes_t, rw_t, wqv, wkv, wvv, wh, egv, euv, edv,
    xin, tab, kq, ee, vt, rt, mix, res_out, res_in, tok_out, tok_in, lined, spread, sorted_in, gains, plan, dall, xq, chl, rsd, xs, hid,
    send1, recv1, send2, recv2,
    lsem, ssem_in, ag_s, ag_r, ps, pr, a_s, a_r, b_s, b_r,
):
    me = lax.axis_index("ep")
    co = (me // 32, (me // 8) % 4, (me // 2) % 4)
    c = me % 2
    own = co[0] * 4 + co[1]
    n_tok = tokens.shape[0]

    def along(axis, d):
        return ((co[axis] + d) % 4 - co[axis]) * STRIDES[axis]

    line = [(me + along(0, d), ((co[0] + d) % 4, co[1])) for d in (2, 1, 3)]
    cross = [(me + along(1, d), (co[0], (co[1] + d) % 4)) for d in (2, 1, 3)]

    seat = co[2] * 2 + c
    mates = [(me + along(2, d), (co[2] + d) % 4 * 2 + c) for d in (2, 1, 3)]
    mates.append((me + 1 - 2 * c, seat + 1 - 2 * c))
    others = mates + [(there + 1 - 2 * c, its_seat + 1 - 2 * c) for there, its_seat in mates[:3]]

    bar = pltpu.get_barrier_semaphore()
    for there, _ in others:
        pl.semaphore_signal(bar, inc=1, device_id=(there,), device_id_type=MESH)
    for there, _ in line + cross:
        pl.semaphore_signal(bar, inc=1, device_id=(there,), device_id_type=MESH)

    def fetch(n, src, dst):
        cp = pltpu.make_async_copy(src, dst, lsem.at[n])
        cp.start()
        return cp

    cp_tok = fetch(7, tokens_h, tokens)
    cp_mixg = fetch(8, mixg_h, mixg)
    cp_rt = fetch(9, routes_h, routes_t)
    cp_rw = fetch(10, rw_h, rw_t)
    cp_pos = fetch(11, pos_h, pos)
    cp_wo = fetch(0, wo, wh.at[own])
    cp_k = fetch(1, wk, wkv)
    cp_q = fetch(2, wq, wqv)
    cp_v = fetch(3, wv, wvv)

    def state_in(h):
        return pltpu.make_async_copy(state.at[:, h], new_state.at[:, h], ssem_in.at[h])

    for h in range(4):
        state_in(h).start()
    cp_retg = fetch(12, retg_h, retg)
    cp_ffng = fetch(13, ffng_h, ffng)
    cp_rt.wait()
    cp_rw.wait()
    cp_pos.wait()

    tab[...] = jnp.full(tab.shape, -1, jnp.int32)
    tab[0:6, 0:n_tok] = routes_t[...]
    tab[8:9, 0:n_tok] = pos[...]
    wtab = jnp.concatenate([rw_t[...], jnp.zeros((6, 128 - n_tok), F32)], axis=1)
    rows = lax.broadcasted_iota(jnp.int32, (256, 128), 0)
    expert = rows // 2
    slot = (rows % 2).astype(F32)
    member = jnp.zeros((256, 128), F32)
    weight = jnp.zeros((256, 128), F32)
    for k in range(6):
        hit = tab[k : k + 1, :] == expert
        member = member + jnp.where(hit, 1.0, 0.0)
        weight = weight + jnp.where(hit, wtab[k : k + 1, :], 0.0)
    before = jnp.where(
        lax.broadcasted_iota(jnp.int32, (128, 128), 0) < lax.broadcasted_iota(jnp.int32, (128, 128), 1), 1.0, 0.0
    ).astype(BF)
    place = jnp.dot(member.astype(BF), before, preferred_element_type=F32)
    chosen = jnp.where(place == slot, member, 0.0)
    plan[seat] = jnp.full((8, 128), -1.0, F32)
    plan[seat, 0:6, 0:n_tok] = routes_t[...].astype(F32)
    comb = (chosen * weight).T
    high = comb.astype(BF)
    chl[0:32, :] = high[0:32, :]
    chl[32:64, :] = (comb - high.astype(F32)).astype(BF)[0:32, :]

    erow = lax.broadcasted_iota(jnp.int32, (128, 128), 0)
    etok = jnp.where(erow < 64, erow % 32, -1)
    for t in range(n_tok):
        ee[:, t * 128 : (t + 1) * 128] = jnp.where(etok == t, 1.0, 0.0).astype(BF)

    spots = tab[8:9, 0:32].astype(F32)
    freqs = jnp.exp(-math.log(10000.0) * lax.broadcasted_iota(jnp.int32, (32, 32), 0).astype(F32) / 32.0)
    angle = spots * freqs
    cosine = jnp.cos(angle)
    sine = jnp.sin(angle)

    cp_tok.wait()
    cp_mixg.wait()
    wide = tokens[...].astype(F32)
    scaled = wide * lax.rsqrt(jnp.mean(wide * wide, axis=-1, keepdims=True) + EPS)
    xin[...] = jnp.zeros(xin.shape, BF)
    xin[0:n_tok, :] = (scaled * mixg[...]).astype(BF)

    def send_block(cc, part, peers, sem):
        piece = wh.at[cc[0] * 4 + cc[1], :, pl.ds(part * 512, 512)]
        for there, _ in peers:
            pltpu.make_async_remote_copy(
                src_ref=piece, dst_ref=piece, send_sem=ag_s, recv_sem=ag_r.at[sem],
                device_id=(there,), device_id_type=MESH,
            ).start()

    def gathered(n, sem):
        seen = wh.at[pl.ds(0, n), :, pl.ds(0, 512)]
        pltpu.make_async_copy(seen, seen, ag_r.at[sem]).wait()

    def gather_start():
        here = (co[0], co[1])
        send_block(here, 0, line, 0)
        send_block(here, 1, cross, 1)
        send_block(here, 0, cross, 2)
        send_block(here, 1, line, 3)

    def gather_forward():
        gathered(3, 0)
        for _, cc in line:
            send_block(cc, 0, cross, 2)
        gathered(3, 1)
        for _, cc in cross:
            send_block(cc, 1, line, 3)

    def project(wref, n):
        return jnp.dot(xin[...], wref[:, n * 256 : (n + 1) * 256], preferred_element_type=F32).astype(BF).astype(F32)

    def rotated(offset, wref, scale):
        for n in range(2):
            cols = project(wref, n).T
            for s in range(4):
                a = cols[s * 64 : s * 64 + 32, :]
                b = cols[s * 64 + 32 : s * 64 + 64, :]
                for first, value in ((0, a * cosine - b * sine), (32, b * cosine + a * sine)):
                    value = value * scale
                    high = value.astype(BF)
                    low_part = (value - high.astype(F32)).astype(BF)
                    kq[n * 4 + s, offset + first : offset + first + 32, :] = jnp.concatenate(
                        [high, low_part, jnp.zeros((32, 64), BF)], axis=1
                    )

    cp_k.wait()
    rotated(0, wkv, 0.125)
    pl.semaphore_wait(bar, 13)
    cp_wo.wait()
    gather_start()
    for there, _ in others:
        pltpu.make_async_remote_copy(
            src_ref=plan.at[seat], dst_ref=plan.at[seat], send_sem=ps.at[3], recv_sem=pr.at[7],
            device_id=(there,), device_id_type=MESH,
        ).start()
    for h in range(4, 8):
        state_in(h).start()
    cp_q.wait()
    rotated(64, wqv, 1.0)
    cp_v.wait()
    for n in range(4):
        part = project(wvv, n)
        vt[2 * n] = part[:, 0:128]
        vt[2 * n + 1] = part[:, 128:256]

    def seven(buf, sem):
        seen = buf.at[pl.ds(0, 7), pl.ds(0, 24)]
        pltpu.make_async_copy(seen, seen, sem).wait()

    def two_heads(p):
        for h in (2 * p, 2 * p + 1):
            state_in(h).wait()
        lhs = kq[2 * p : 2 * p + 2].reshape(256, 128)
        for g in range(n_tok // 4):
            wide_kq = jnp.dot(lhs, ee[:, g * 512 : (g + 1) * 512], preferred_element_type=F32)
            for n, h in enumerate((2 * p, 2 * p + 1)):
                decay = 1.0 - 2.0 ** (-2 - h)
                for i in range(4):
                    t = g * 4 + i
                    key = wide_kq[n * 128 : n * 128 + 64, i * 128 : (i + 1) * 128]
                    query = wide_kq[n * 128 + 64 : n * 128 + 128, i * 128 : (i + 1) * 128]
                    new = decay * new_state[t, h] + key * vt[h, t : t + 1, :]
                    new_state[t, h] = new
                    rt[h, t : t + 1, :] = jnp.sum(query * new, axis=0, keepdims=True)
        for h in (2 * p, 2 * p + 1):
            read = rt[h, 0:n_tok, :]
            centred = read - jnp.mean(read, axis=-1, keepdims=True)
            normed = centred * lax.rsqrt(jnp.mean(centred * centred, axis=-1, keepdims=True) + EPS)
            mix[seat, 0:n_tok, h * 128 : (h + 1) * 128] = (normed * retg[:, h * 128 : (h + 1) * 128]).astype(BF)
        piece = mix.at[seat, pl.ds(0, 24), pl.ds(p * 256, 256)]
        for n, (there, _) in enumerate(mates):
            pltpu.make_async_remote_copy(
                src_ref=piece, dst_ref=piece, send_sem=ps.at[0], recv_sem=pr.at[2 + (0, 2, 1, 3)[n]],
                device_id=(there,), device_id_type=MESH,
            ).start()

    cp_retg.wait()
    two_heads(0)
    two_heads(1)
    two_heads(2)
    gather_forward()
    two_heads(3)
    cp_g = fetch(4, eg.at[0], egv)
    cp_u = fetch(5, eu.at[0], euv)
    cp_d = fetch(6, ed.at[0], edv)

    srow = lax.broadcasted_iota(jnp.int32, (1024, 128), 0)
    lane = lax.broadcasted_iota(jnp.int32, (1024, 128), 1)
    target = srow % 128 // 16 * 128 + srow // 128 * 16 + srow % 16
    for n in range(8):
        spread[:, n * 128 : (n + 1) * 128] = jnp.where(lane + n * 128 == target, 1.0, 0.0).astype(BF)

    cp_ffng.wait()
    sorted_in[0:n_tok, :] = tokens[:, 0:1024]
    sorted_in[32 : 32 + n_tok, :] = tokens[:, 1024:2048]
    rows = []
    for n in range(2):
        rest = ffng[:, n * 1024 : (n + 1) * 1024]
        for _ in range(3):
            piece = rest.astype(BF).astype(F32)
            rows.append(piece)
            rest = rest - piece
    rows.append(jnp.zeros((10, 1024), F32))
    sorted_in[64:80, :] = jnp.concatenate(rows, axis=0).astype(BF)
    by_core = lax.dot_general(sorted_in[...], spread[...], (((1,), (1,)), ((), ())), preferred_element_type=F32)
    for g in range(8):
        for n in range(2):
            part = by_core[:, g * 128 : (g + 1) * 128]
            tok_out[g, :, n * 128 : (n + 1) * 128] = part[n * 32 : n * 32 + 32, :].astype(BF)
            at = 64 + 3 * n
            gains[g : g + 1, n * 128 : (n + 1) * 128] = part[at : at + 1, :] + part[at + 1 : at + 2, :] + part[at + 2 : at + 3, :]
    for there, its_seat in others:
        pltpu.make_async_remote_copy(
            src_ref=tok_out.at[its_seat, pl.ds(0, 24)], dst_ref=tok_in.at[seat, pl.ds(0, 24)],
            send_sem=ps.at[2], recv_sem=pr.at[6], device_id=(there,), device_id_type=MESH,
        ).start()
    tok_in[seat] = tok_out[seat]
    routed = plan.at[pl.ds(0, 7)]
    pltpu.make_async_copy(routed, routed, pr.at[7]).wait()
    ids = jnp.concatenate([plan[g, :, 0:32] for g in range(8)], axis=1)
    mrow = lax.broadcasted_iota(jnp.int32, (256, 256), 0)
    mlane = lax.broadcasted_iota(jnp.int32, (256, 256), 1)
    mine_f = jnp.where(mrow % 16 // 2 == mlane // 32, 1.0, 0.0)
    slot_f = (mrow % 2).astype(F32)
    expert_f = (mrow // 16).astype(F32)
    earlier = jnp.where(mrow < mlane, 1.0, 0.0).astype(BF)
    for b in range(8):
        member = jnp.zeros((256, 256), F32)
        shifted_ids = ids - 16.0 * b
        for k in range(6):
            member = jnp.where(shifted_ids[k : k + 1, :] == expert_f, mine_f, member)
        place = jnp.dot(member.astype(BF), earlier, preferred_element_type=F32)
        dall[b * 256 : (b + 1) * 256, :] = jnp.where(place == slot_f, member, 0.0).astype(BF)
    for n in (1, 2, 0):
        its_seat = mates[n][1]
        block = mix.at[0, pl.ds(0, 24)]
        pltpu.make_async_copy(block, block, pr.at[2 + n]).wait()
        block = mix.at[its_seat, pl.ds(0, 24)]
        pltpu.make_async_remote_copy(
            src_ref=block, dst_ref=block, send_sem=ps.at[0], recv_sem=pr.at[0],
            device_id=(mates[3][0],), device_id_type=MESH,
        ).start()
    gathered(12, 2)
    gathered(12, 3)
    block = mix.at[0, pl.ds(0, 24)]
    pltpu.make_async_copy(block, block, pr.at[5]).wait()
    pltpu.make_async_copy(mix.at[pl.ds(0, 3), pl.ds(0, 24)], mix.at[pl.ds(0, 3), pl.ds(0, 24)], pr.at[0]).wait()
    seven(tok_in, pr.at[6])
    attended = lax.dot_general(
        mix[...].reshape(256, 1024), wh[...].reshape(256, 1024), (((1,), (1,)), ((), ())), preferred_element_type=F32
    ).astype(BF).astype(F32)
    piece = (tok_in[...].reshape(256, 256).astype(F32) + attended).astype(BF).astype(F32)
    real = lax.broadcasted_iota(jnp.int32, (256, 256), 0) % 32 < n_tok
    piece = jnp.where(real, piece, 0.0).astype(BF)
    res_out[...] = piece.reshape(8, 32, 256)
    for b in range(8):
        out = jnp.dot(dall[b * 256 : (b + 1) * 256, :], piece, preferred_element_type=F32)
        send1[b * 16 : (b + 1) * 16] = out.astype(BF).reshape(16, 16, 256)

    def peers(half, sign, put):
        zs = [(co[0] + sign * d) % 4 * 32 for d in range(4)]
        ys = [(co[1] + sign * d) % 4 * 8 for d in range(4)]
        xs4 = [(co[2] + sign * d) % 4 * 2 for d in range(4)]
        cs = [c, 1 - c]
        for l, dz, dy, dx, dc in MOVES[half]:
            its_seat = xs4[dx] + cs[dc]
            put(l, its_seat, zs[dz] + ys[dy] + its_seat)

    def dispatch(half):
        def put(l, its_seat, t):
            pltpu.make_async_remote_copy(
                src_ref=send1.at[t], dst_ref=recv1.at[seat, pl.ds(l * 16, 16)], send_sem=a_s, recv_sem=a_r.at[half],
                device_id=(t,), device_id_type=MESH,
            ).start()

        peers(half, 1, put)

    def give_back(half):
        def put(l, its_seat, t):
            pltpu.make_async_remote_copy(
                src_ref=send2.at[l * 8 + its_seat], dst_ref=recv2.at[me], send_sem=b_s, recv_sem=b_r,
                device_id=(t,), device_id_type=MESH,
            ).start()

        peers(half, -1, put)

    def arrived(buf, first, count, sem):
        seen = buf.at[pl.ds(first, count)]
        pltpu.make_async_copy(seen, seen, sem).wait()

    def experts(half):
        first, n_rows = BOUNDS[half] * 16, (BOUNDS[half + 1] - BOUNDS[half]) * 16
        mine = slice(first, first + n_rows)
        square = jnp.zeros((n_rows, 128), F32)
        for g in range(8):
            value = recv1[g, mine, :].astype(F32)
            value = value * value
            square = square + value[:, 0:128] + value[:, 128:256]
        inv = lax.rsqrt(jnp.sum(square, axis=-1, keepdims=True) / 2048.0 + EPS)
        for g in range(8):
            xq[g, 0:n_rows, :] = (recv1[g, mine, :].astype(F32) * inv * gains[g : g + 1, :]).astype(BF)

        def rows_of(ref, g, cols):
            return jnp.concatenate([ref[n * 128 + g * 16 : n * 128 + g * 16 + 16, cols] for n in range(16)], axis=0)

        for n in range(2):
            cols = slice(n * 256, (n + 1) * 256)
            gate = jnp.zeros((n_rows, 256), F32)
            up = jnp.zeros((n_rows, 256), F32)
            for g in range(8):
                gate = gate + jnp.dot(xq[g, 0:n_rows, :], rows_of(egv, g, cols), preferred_element_type=F32)
                up = up + jnp.dot(xq[g, 0:n_rows, :], rows_of(euv, g, cols), preferred_element_type=F32)
            hid[mine, cols] = (jax.nn.silu(gate) * up).astype(BF)
        for n in range(8):
            cols = slice(n * 256, (n + 1) * 256)
            out = jnp.dot(hid[mine, :], edv[:, cols], preferred_element_type=F32).astype(BF)
            send2[first // 2 : (first + n_rows) // 2, :, cols] = out.reshape(n_rows // 2, 2, 256)

    for n in range(len(MOVES)):
        dispatch(n)
    recv1[seat, 0:16, :] = send1[me]
    for there, its_seat in others:
        pltpu.make_async_remote_copy(
            src_ref=res_out.at[its_seat, pl.ds(0, 24)], dst_ref=res_in.at[seat, pl.ds(0, 24)],
            send_sem=ps.at[1], recv_sem=pr.at[1], device_id=(there,), device_id_type=MESH,
        ).start()
    res_in[seat] = res_out[seat]
    cp_g.wait()
    cp_u.wait()
    cp_d.wait()
    arrived(send1, 0, 63, a_r.at[0])
    experts(0)
    give_back(0)
    recv2[me] = send2[seat]
    arrived(send1, 0, 64, a_r.at[1])
    experts(1)
    give_back(1)
    seven(res_in, pr.at[1])
    for n in range(2):
        for g in range(8):
            lined[n * 32 : (n + 1) * 32, g * 128 : (g + 1) * 128] = res_in[g, :, n * 128 : (n + 1) * 128]
    resid = jnp.dot(lined[...], spread[...], preferred_element_type=F32)
    rsd[:, 0:1024] = resid[0:n_tok, :]
    rsd[:, 1024:2048] = resid[32 : 32 + n_tok, :]
    arrived(recv2, 0, 127, b_r)

    def unpack2(i, _):
        xs[pl.ds(i * 16, 16), :] = recv2[pl.ds(i * 8, 8)].reshape(16, 2048)
        return 0

    lax.fori_loop(0, 16, unpack2, 0)
    for n in range(8):
        cols = slice(n * 256, (n + 1) * 256)
        got = jnp.dot(chl[...], xs[:, cols], preferred_element_type=F32)
        result[:, cols] = (rsd[:, cols] + got[0:n_tok, :] + got[32 : 32 + n_tok, :]).astype(BF)

    arrived(send1, 0, 127, a_s)
    arrived(send2, 0, 127, b_s)
    sent = wh.at[pl.ds(0, 15)]
    pltpu.make_async_copy(sent, sent, ag_s).wait()
    seven(mix, ps.at[0])
    seven(res_out, ps.at[1])
    seven(tok_out, ps.at[2])
    pltpu.make_async_copy(routed, routed, ps.at[3]).wait()


def hand_over(result, new_state, result_out, state_out, sems):
    copies = [pltpu.make_async_copy(result, result_out, sems.at[10])]
    for n in range(10):
        rows = pl.ds(n * 2, 2)
        copies.append(pltpu.make_async_copy(new_state.at[rows], state_out.at[rows], sems.at[n]))
    for cp in copies:
        cp.start()
    for cp in copies:
        cp.wait()


def shards(
    tokens, positions, state, mix_gain, w_query, w_key, w_value, ret_gain, w_out, ffn_gain,
    routes, route_weights, expert_gate, expert_up, expert_down,
):
    vmem = pl.BlockSpec(memory_space=pltpu.VMEM)
    hbm = pl.BlockSpec(memory_space=pl.ANY)
    n_tok = tokens.shape[0]
    dma = pltpu.SemaphoreType.DMA
    vm = pltpu.VMEM
    result, new_state = pl.pallas_call(
        kernel,
        out_shape=(
            pltpu.VMEM(tokens.shape, BF),
            pltpu.VMEM(state.shape, F32),
        ),
        in_specs=[hbm] * 15,
        out_specs=(vmem, vmem),
        scratch_shapes=[
            vm((n_tok, 2048), BF), vm((1, n_tok), jnp.int32), vm((1, 2048), F32), vm((1, 1024), F32), vm((1, 2048), F32),
            vm((6, n_tok), jnp.int32), vm((6, n_tok), F32),
            vm((2048, 512), BF), vm((2048, 512), BF), vm((2048, 1024), BF),
            vm((16, 16, 1024), BF), vm((2048, 512), BF), vm((2048, 512), BF), vm((512, 2048), BF),
            vm((32, 2048), BF), vm((16, 128), jnp.int32), vm((8, 128, 128), BF), vm((128, n_tok * 128), BF),
            vm((8, 32, 128), F32), vm((8, 32, 128), F32), vm((8, 32, 1024), BF),
            vm((8, 32, 256), BF), vm((8, 32, 256), BF), vm((8, 32, 256), BF), vm((8, 32, 256), BF),
            vm((64, 1024), BF), vm((1024, 1024), BF), vm((80, 1024), BF), vm((8, 256), F32), vm((8, 8, 128), F32),
            vm((2048, 256), BF), vm((8, 128, 256), BF), vm((64, 256), BF),
            vm((n_tok, 2048), F32), vm((256, 2048), BF), vm((256, 512), BF),
            vm((128, 16, 256), BF), vm((8, 256, 256), BF), vm((128, 2, 2048), BF), vm((128, 2, 2048), BF),
            dma((14,)), dma((8,)), dma, dma((4,)), dma((4,)), dma((8,)), dma, dma((2,)), dma, dma,
        ],
        compiler_params=pltpu.CompilerParams(collective_id=0, has_side_effects=True, vmem_limit_bytes=61650000),
        name="layer",
    )(
        tokens, positions.reshape(1, n_tok), mix_gain.reshape(1, -1), ret_gain.reshape(1, -1), ffn_gain.reshape(1, -1),
        routes.T, route_weights.T, state, w_query, w_key, w_value, w_out.T, expert_gate, expert_up, expert_down,
    )
    return pl.pallas_call(
        hand_over,
        out_shape=(jax.ShapeDtypeStruct(tokens.shape, BF), jax.ShapeDtypeStruct(state.shape, F32)),
        in_specs=[vmem] * 2,
        out_specs=(hbm, hbm),
        scratch_shapes=[dma((11,))],
        compiler_params=pltpu.CompilerParams(vmem_limit_bytes=1 << 20),
        name="hand_over",
    )(result, new_state)


def solution(mesh):
    placed = (
        P("ep", None), P("ep"), P("ep", None, None, None), P(), P(), P(), P(), P(), P(None, "ep"), P(),
        P("ep", None), P("ep", None), P("ep", None, None), P("ep", None, None), P("ep", None, None),
    )
    return jax.shard_map(
        shards, mesh=mesh, in_specs=placed, out_specs=(P("ep", None), P("ep", None, None, None)), check_vma=False
    )
```
